512 devices in a mesh: row: 32 (over z, core), col: 16 (over y, x).
Axes of the slice: x: 4, y: 4, z: 16, core: 2. Of those that a mesh axis runs over, the one named last changes fastest.
Arguments:
- tokens: bfloat16 [1, 8192, 2048], P(None, 'row'), may hold values from -6 to 6
- w_value: bfloat16 [2048, 1024], P(None, 'col'), may hold values from -0.125 to 0.125
- w_first: bfloat16 [2048, 1024], P(None, 'col'), may hold values from -0.125 to 0.125
- w_second: bfloat16 [2048, 1024], P(None, 'col'), may hold values from -0.125 to 0.125
- w_gate: bfloat16 [2048, 1024], P(None, 'col'), may hold values from -0.125 to 0.125
- conv_taps: float32 [3, 3, 1024], P(None, None, 'col'), may hold values from -3.5 to 3.5
- filter_embed: float32 [33, 64], replicated, may hold values from -192 to 192
- filter_freq: float32 [64], replicated, may hold values from 0.1 to 1.9
- filter_proj: float32 [64, 2, 2, 1024], P(None, None, None, 'col'), may hold values from -0.01171875 to 0.01171875
- filter_decay: float32 [2, 2, 1024], P(None, None, 'col'), may hold values from 0.25 to 128
- skip_gain: float32 [2, 1024], P(None, 'col'), may hold values from -3 to 3
- w_out: bfloat16 [1024, 2048], P('col'), may hold values from -0.1875 to 0.1875
Outputs:
- mixed: bfloat16 [1, 8192, 2048], P(None, ('row', 'col'))
The draws below stay inside these ranges and needn't reach their ends.
All inputs are finite; a program needn't handle non-finite values.
Results may differ from the reference program's by a relative error of at most 0.018.
Values may be sent and summed in bfloat16 or wider, within the bound.
A program may use at most 64 MiB of HBM per device.

```python
import math
import jax
import jax.numpy as jnp
from jax import lax

D = 2048
C = 1024
HID = 64
EMB = 33
SEQS = 1
SEQ_LEN = 8192


def levels(stream_key, shape, pieces, low, largest):
    loudness = 1.0
    for position, parts in pieces:
        steps = jax.random.uniform(jax.random.fold_in(jax.random.fold_in(stream_key, 6), position), (parts,), jnp.float32, low / len(pieces), largest / len(pieces))
        loudness = loudness * jnp.repeat(jnp.exp(steps), shape[position] // parts).reshape((-1,) + (1,) * (len(shape) - 1 - position))
    return loudness


def gaussian(own_key, shape, scale, limit, shards=(), held_as=jnp.bfloat16):
    values = scale * jax.random.normal(own_key, shape, jnp.float32)
    if shards:
        values = values * levels(own_key, shape, shards, -0.22, 0.18)
    return jnp.clip(values, -limit, limit).astype(held_as)


def setup_inputs(seed: int = 0) -> dict:
    key_of = jax.random.split(jax.random.key(seed), 13)
    return {
        "tokens": gaussian(key_of[0], (SEQS, SEQ_LEN, D), 1.0, 6.0, ((1, 32),)),
        "w_value": gaussian(key_of[1], (D, C), D ** -0.5, 0.125, ((1, 16),)),
        "w_first": gaussian(key_of[2], (D, C), D ** -0.5, 0.125, ((1, 16),)),
        "w_second": gaussian(key_of[3], (D, C), D ** -0.5, 0.125, ((1, 16),)),
        "w_gate": gaussian(key_of[4], (D, C), D ** -0.5, 0.125, ((1, 16),)),
        "conv_taps": gaussian(key_of[5], (3, 3, C), 3 ** -0.5, 3.5, ((2, 16),), jnp.float32),
        "filter_embed": gaussian(key_of[6], (EMB, HID), (max(1, SEQ_LEN // 256)), 192.0, (), jnp.float32),
        "filter_freq": jnp.clip(1.0 + 0.18 * jax.random.normal(key_of[7], (HID,), jnp.float32), 0.1, 1.9),
        "filter_proj": gaussian(key_of[8], (HID, 2, 2, C), (HID * SEQ_LEN // 2) ** -0.5, 0.01171875, ((3, 16),), jnp.float32),
        "filter_decay": jnp.clip(jnp.exp(math.log(128.0) - 6.2383246 * jax.random.uniform(key_of[9], (2, 2, C), jnp.float32) ** levels(key_of[9], (2, 2, C), ((2, 16),), -0.2, 0.2)), 0.25, 128.0),
        "skip_gain": gaussian(key_of[10], (2, C), 0.5, 3.0, ((1, 16),), jnp.float32),
        "w_out": gaussian(key_of[11], (C, D), C ** -0.5, 0.1875, ((0, 16),)),
    }


def filter_spectra(length, filter_embed, filter_freq, filter_proj, filter_decay):
    bands = (filter_embed.shape[0] - 1) // 2
    index = jnp.arange(length, dtype=jnp.int32)
    spot = index.astype(jnp.float32) / (length - 1)
    freqs = jnp.arange(1, bands + 1, dtype=jnp.int32)
    phase = ((index[:, None] * freqs[None, :]) % length).astype(jnp.float32) * (2.0 * math.pi / length)
    features = jnp.concatenate([spot[:, None], jnp.cos(phase), jnp.sin(phase)], axis=1)
    hidden = jnp.sin(filter_freq[None, :] * jnp.dot(features, filter_embed, precision=lax.Precision.HIGHEST))
    width = filter_proj.shape[3]
    taps = jnp.dot(hidden, filter_proj.reshape(filter_proj.shape[0], 4 * width), precision=lax.Precision.HIGHEST)
    taps = taps.reshape(length, 2, 2, width) * jnp.exp(-spot[:, None, None, None] * filter_decay[None])
    spectra = []
    for order in range(2):
        ahead = taps[:, order, 0]
        behind = taps[:, order, 1]
        cycle = jnp.concatenate([ahead, jnp.zeros((1, width), jnp.float32), behind[1:][::-1]], axis=0)
        spectra.append(jnp.fft.rfft(cycle, axis=0))
    return spectra


def long_conv(signal, spectrum, gain):
    length = signal.shape[0]
    signal_spec = jnp.fft.rfft(signal, n=2 * length, axis=0)
    result = jnp.fft.irfft(signal_spec * spectrum, n=2 * length, axis=0)[:length]
    return result + gain[None, :] * signal


def one_sequence(sequence, w_value, w_first, w_second, w_gate, conv_taps, spectra, skip_gain, w_out):
    width = w_value.shape[1]
    proj = jnp.concatenate([jnp.dot(sequence, w_value, preferred_element_type=jnp.float32),
                            jnp.dot(sequence, w_first, preferred_element_type=jnp.float32),
                            jnp.dot(sequence, w_second, preferred_element_type=jnp.float32)], axis=1).astype(jnp.bfloat16)
    gate = jnp.dot(sequence, w_gate, preferred_element_type=jnp.float32).astype(jnp.bfloat16)
    padded = jnp.pad(proj, ((1, 1), (0, 0))).astype(jnp.float32)
    weights = conv_taps.reshape(3, 3 * width)
    short = padded[:-2] * weights[0] + padded[1:-1] * weights[1] + padded[2:] * weights[2]
    value = short[:, :width]
    first = short[:, width:2 * width]
    second = short[:, 2 * width:]
    inner = first * long_conv(value, spectra[0], skip_gain[0])
    outer = (second * long_conv(inner, spectra[1], skip_gain[1]) * jax.nn.silu(gate.astype(jnp.float32))).astype(jnp.bfloat16)
    return jnp.dot(outer, w_out, preferred_element_type=jnp.float32).astype(jnp.bfloat16)


def reference(tokens, w_value, w_first, w_second, w_gate, conv_taps, filter_embed, filter_freq, filter_proj, filter_decay, skip_gain, w_out):
    length = tokens.shape[1]
    spectra = filter_spectra(length, filter_embed, filter_freq, filter_proj, filter_decay)
    results = [one_sequence(tokens[number], w_value, w_first, w_second, w_gate, conv_taps, spectra, skip_gain, w_out)
               for number in range(tokens.shape[0])]
    return jnp.stack(results, axis=0)
```

```python
import functools
import math

import jax
import jax.numpy as jnp
import ml_dtypes
import numpy as np
from jax import lax
from jax.experimental import pallas as pl
from jax.experimental.pallas import tpu as pltpu
from jax.sharding import PartitionSpec as P

MESH = pl.DeviceIdType.MESH
F32 = jnp.float32
BF16 = jnp.bfloat16

LENGTH = 8192
ROWS = 32
COLS = 16
FEATS = 33
FEAT_STEP = 40


def halves(x):
    x = np.asarray(x, np.float64)
    high = x.astype(ml_dtypes.bfloat16)
    low = (x - high.astype(np.float64)).astype(ml_dtypes.bfloat16)
    return high, low


@functools.lru_cache(None)
def constants():
    two_pi = 2.0 * math.pi
    j = np.arange(64)
    q = 2 * (j % 32) + j // 32
    k1 = np.arange(64) + 0.5
    p = np.arange(128)
    first = np.concatenate([np.cos(two_pi * np.outer(k1, q) / 128), -np.sin(two_pi * np.outer(k1, q) / 128)], axis=0)
    f_high, f_low = halves(first)
    outer_in = np.concatenate([f_high, f_high, f_low], axis=1)
    outer_out = np.concatenate([f_high.T, f_high.T, f_low.T], axis=1)
    twist = np.stack(
        [np.cos(two_pi * np.outer(k1, p) / 16384), -np.sin(two_pi * np.outer(k1, p) / 16384)]
    ).astype(np.float32)
    g_real = np.cos(two_pi * (np.outer(p, p) % 128) / 128)
    g_imag = -np.sin(two_pi * (np.outer(p, p) % 128) / 128)
    inner_in = np.stack(halves(np.block([[g_real, g_imag], [-g_imag, g_real]])))
    inner_out = np.stack(halves(np.block([[g_real, -g_imag], [g_imag, g_real]])))
    n = np.arange(LENGTH)
    b = np.arange(1, 17)
    phase = two_pi * (np.outer(b, n) % LENGTH) / LENGTH
    features = np.concatenate([(n / (LENGTH - 1))[None], np.cos(phase), np.sin(phase)], axis=0)
    table = np.zeros((128, LENGTH), ml_dtypes.bfloat16)
    rest = features
    for part in range(3):
        piece = rest.astype(ml_dtypes.bfloat16)
        table[part * FEAT_STEP : part * FEAT_STEP + FEATS] = piece
        rest = rest - piece.astype(np.float64)
    return outer_in, outer_out, twist, inner_in, inner_out, table


def split(x):
    high = x.astype(BF16)
    return high, (x - high.astype(F32)).astype(BF16)


def dot(a, b):
    return jnp.dot(a, b, preferred_element_type=F32)


def dot_nt(a, b, precision=None):
    return lax.dot_general(a, b, (((1,), (1,)), ((), ())), precision=precision, preferred_element_type=F32)


def times(x, matrix):
    high, low = split(x)
    return dot(high, matrix[0]) + dot(low, matrix[0]) + dot(high, matrix[1])


def forward(signal, outer_in, twist, inner_in):
    high, low = split(signal)
    stage = dot(outer_in, jnp.concatenate([high, low, high], axis=0))
    turned = []
    for m in range(signal.shape[1] // 128):
        real = stage[:64, 128 * m : 128 * (m + 1)]
        imag = stage[64:, 128 * m : 128 * (m + 1)]
        turned.append(
            jnp.concatenate([real * twist[0] - imag * twist[1], real * twist[1] + imag * twist[0]], axis=1)
        )
    return times(jnp.concatenate(turned, axis=0), inner_in)


def inverse(spectrum, outer_out, twist, inner_out):
    stage = times(spectrum, inner_out)
    reals, imags = [], []
    for m in range(spectrum.shape[0] // 64):
        real = stage[64 * m : 64 * (m + 1), :128]
        imag = stage[64 * m : 64 * (m + 1), 128:]
        reals.append(real * twist[0] + imag * twist[1])
        imags.append(imag * twist[0] - real * twist[1])
    both = jnp.concatenate([jnp.concatenate(reals, axis=1), jnp.concatenate(imags, axis=1)], axis=0)
    high, low = split(both)
    return dot(outer_out, jnp.concatenate([high, low, high], axis=0))


def convolve(signal, filt, tables):
    outer_in, outer_out, twist, inner_in, inner_out = tables
    spectrum = forward(signal, outer_in, twist, inner_in)
    real, imag = spectrum[:, :128], spectrum[:, 128:]
    f_real, f_imag = filt[:, :128], filt[:, 128:]
    product = jnp.concatenate([real * f_real - imag * f_imag, real * f_imag + imag * f_real], axis=1)
    return inverse(product, outer_out, twist, inner_out)


def filter_spectrum(signals, outer_in, twist, inner_in):
    spectra = forward(signals, outer_in, twist, inner_in)
    ahead, behind = spectra[:128], spectra[128:]
    scale = 2.0 / (2 * LENGTH)
    return jnp.concatenate(
        [(ahead[:, :128] + behind[:, :128]) * scale, (ahead[:, 128:] - behind[:, 128:]) * scale], axis=1
    )


def sine(x):
    k = jnp.floor(x * (1.0 / math.pi) + 0.5)
    r = x - k * 3.140625
    r = r - k * 9.67502593994140625e-4
    r = r - k * 1.509957990978376432e-7
    half = k * 0.5
    sign = 1.0 - 4.0 * (half - jnp.floor(half))
    s = r * r
    poly = -1.0 / 39916800.0
    for c in (1.0 / 362880.0, -1.0 / 5040.0, 1.0 / 120.0, -1.0 / 6.0):
        poly = poly * s + c
    return sign * (r + r * (s * poly))


def shifted(parts, lane, sub):
    right = [pltpu.roll(x, 1, 1) for x in parts]
    left = [pltpu.roll(x, 127, 1) for x in parts]
    carry = jnp.where(sub == 0, 0.0, pltpu.roll(right[1], 1, 0))
    back = jnp.where(sub == 31, 0.0, pltpu.roll(left[0], 31, 0))
    before = [jnp.where(lane == 0, carry, right[0]), jnp.where(lane == 0, right[0], right[1])]
    after = [jnp.where(lane == 127, left[1], left[0]), jnp.where(lane == 127, back, left[1])]
    return before, after


def kernel(
    tokens, w_value, w_first, w_second, w_gate, conv_taps, embed, freq, proj, decay, gain, w_out,
    outer_in_h, outer_out_h, twist_h, inner_in_h, inner_out_h, table_h,
    out_ref,
    tok_v, w_v, taps_v, embed_v, freq_v, proj_v, decay_v, gain_v,
    outer_in_v, outer_out_v, twist_v, inner_in_v, inner_out_v, table_v,
    w_full, est, lag_taps, spectra, grid_v, send1, recv1, send2, recv2, back_v, send3, recv3, block_v, send4, recv4,
    load_sem, send_sem1, recv_sem1, send_sem2, recv_sem2, send_sem3, recv_sem3, send_sem4, recv_sem4,
    send_sem5, recv_sem5, swap_send, swap_recv,
):
    row = lax.axis_index("row")
    col = lax.axis_index("col")
    z = lax.div(row, 2)
    core = lax.rem(row, 2)
    partner = z * 2 + 1 - core

    def row_peers(visit):
        def step(i, carry):
            away = 8 + lax.div(i + 1, 2) * (1 - 2 * lax.rem(i, 2))
            there = lax.rem(z + away, 16) * 2
            visit(there)
            visit(there + 1)
            return carry

        lax.fori_loop(0, 15, step, 0)
        visit(partner)

    def col_peers(visit):
        def step(i, carry):
            visit(lax.rem(col + i, COLS))
            return carry

        lax.fori_loop(1, COLS, step, 0)

    barrier = pltpu.get_barrier_semaphore()
    row_peers(lambda r: pl.semaphore_signal(barrier, inc=1, device_id=(r, col), device_id_type=MESH))
    col_peers(lambda c: pl.semaphore_signal(barrier, inc=1, device_id=(row, c), device_id_type=MESH))

    own_rows = pl.ds(pl.multiple_of(col * 64, 64), 64)
    loads = []
    for source, target in (
        (tokens.at[0], tok_v),
        (w_value, w_v.at[0]),
        (w_first, w_v.at[1]),
        (w_second, w_v.at[2]),
        (w_gate, w_v.at[3]),
        (w_out.at[:, pl.ds(pl.multiple_of(core * 1024, 1024), 1024)], w_full.at[core, own_rows]),
        (conv_taps, taps_v),
        (embed, embed_v),
        (freq, freq_v),
        (proj, proj_v),
        (decay, decay_v),
        (gain, gain_v),
        (table_h, table_v),
        (outer_in_h, outer_in_v),
        (outer_out_h, outer_out_v),
        (twist_h, twist_v),
        (inner_in_h, inner_in_v),
        (inner_out_h, inner_out_v),
    ):
        load = pltpu.make_async_copy(source, target, load_sem.at[len(loads)])
        load.start()
        loads.append(load)

    for load in loads[:5]:
        load.wait()
    order = lax.broadcasted_iota(jnp.int32, (256, 64), 0)
    channel = lax.broadcasted_iota(jnp.int32, (256, 64), 1)
    own_channel = channel == 2 * (order >> 3) + ((order >> 1) & 1)
    place = [
        jnp.where(own_channel & ((order & 1) == h) & (((order >> 2) & 1) == k), 1.0, 0.0).astype(BF16)
        for k in range(2)
        for h in range(2)
    ]
    for pair, target in ((0, send1), (2, send2)):
        total = jnp.zeros((256, 128), F32)
        for k in range(2):
            result = dot(tok_v[...], w_v[pair + k]).astype(BF16)
            for h in range(2):
                total = total + dot_nt(place[2 * k + h], result[128 * h : 128 * (h + 1)])
        target[...] = total.reshape(ROWS, 8, 128).astype(BF16)
    recv1[pl.ds(row, 1)] = send1[pl.ds(row, 1)]
    recv2[pl.ds(row, 1)] = send2[pl.ds(row, 1)]
    loads[5].wait()

    def to_row(source, target, sent, received, r):
        return pltpu.make_async_remote_copy(
            src_ref=source.at[r], dst_ref=target.at[row], send_sem=sent.at[r], recv_sem=received.at[row],
            device_id=(r, col), device_id_type=MESH,
        )

    def from_row(source, target, sent, received, r):
        return pltpu.make_async_remote_copy(
            src_ref=source.at[r], dst_ref=target.at[r], send_sem=sent.at[r], recv_sem=received.at[r],
            device_id=(r, col), device_id_type=MESH,
        )

    def to_col(source, target, sent, received, c):
        return pltpu.make_async_remote_copy(
            src_ref=source.at[c], dst_ref=target.at[col], send_sem=sent.at[c], recv_sem=received.at[col],
            device_id=(row, c), device_id_type=MESH,
        )

    def from_col(source, target, sent, received, c):
        return pltpu.make_async_remote_copy(
            src_ref=source.at[c], dst_ref=target.at[c], send_sem=sent.at[c], recv_sem=received.at[c],
            device_id=(row, c), device_id_type=MESH,
        )

    def weight_rows(c):
        return w_full.at[core, pl.ds(pl.multiple_of(c * 64, 64), 64)]

    def weights_to(c):
        return pltpu.make_async_remote_copy(
            src_ref=weight_rows(col), dst_ref=weight_rows(col), send_sem=send_sem5.at[c], recv_sem=recv_sem5.at[col],
            device_id=(row, c), device_id_type=MESH,
        )

    def weights_from(c):
        return pltpu.make_async_remote_copy(
            src_ref=weight_rows(c), dst_ref=weight_rows(c), send_sem=send_sem5.at[c], recv_sem=recv_sem5.at[c],
            device_id=(row, c), device_id_type=MESH,
        )

    first_trip = (send1, recv1, send_sem1, recv_sem1)
    second_trip = (send2, recv2, send_sem2, recv_sem2)
    back_trip = (send3, recv3, send_sem3, recv_sem3)
    last_trip = (send4, recv4, send_sem4, recv_sem4)

    pl.semaphore_wait(barrier, ROWS - 1 + COLS - 1)
    row_peers(lambda r: to_row(*first_trip, r).start())
    row_peers(lambda r: to_row(*second_trip, r).start())
    col_peers(lambda c: weights_to(c).start())

    for load in loads[6:]:
        load.wait()
    scaled = embed_v[...] * freq_v[...]
    est[...] = jnp.zeros_like(est)
    high = scaled.astype(BF16).astype(F32)
    rest = scaled - high
    mid = rest.astype(BF16).astype(F32)
    low = rest - mid
    for k, parts in enumerate(((high, high, high), (mid, mid), (low,))):
        for m, part in enumerate(parts):
            est[k, FEAT_STEP * m : FEAT_STEP * m + FEATS, :64] = part
    layer = jnp.concatenate([jnp.transpose(est[k])[:64] for k in range(3)], axis=0).astype(BF16)

    lane64 = lax.broadcasted_iota(jnp.int32, (8, 64), 1)
    sub64 = lax.broadcasted_iota(jnp.int32, (8, 64), 0)
    own_proj = jnp.zeros((8, 64), F32)
    for o in range(2):
        for d in range(2):
            pick = jnp.where((lane64 == 2 * row + (sub64 & 1)) & ((sub64 >> 1) == 2 * o + d), 1.0, 0.0)
            own_proj = own_proj + dot_nt(pick, proj_v[:, o, d, :], lax.Precision.HIGHEST)
    proj_high, proj_low = split(own_proj)
    proj_both = jnp.concatenate([own_proj, own_proj - proj_high.astype(F32)], axis=0).astype(BF16)

    def own(ref):
        lanes = lax.broadcasted_iota(jnp.int32, ref.shape, len(ref.shape) - 1)
        return [jnp.sum(jnp.where(lanes == 2 * row + c, ref[...], 0.0), axis=-1, keepdims=True) for c in range(2)]

    own_taps = own(taps_v)
    own_decay = own(decay_v)
    own_gain = own(gain_v)
    sub8 = lax.broadcasted_iota(jnp.int32, (8, 128), 0)
    decay_rows = jnp.zeros((8, 128), F32)
    start_rows = jnp.zeros((8, 128), F32)
    for o in range(2):
        for c in range(2):
            start_rows = jnp.where(sub8 == 4 * o + c, own_gain[c][o : o + 1], start_rows)
            for d in range(2):
                decay_rows = jnp.where(sub8 == 4 * o + 2 * d + c, own_decay[c][o, d : d + 1], decay_rows)
    lag8 = lax.broadcasted_iota(jnp.int32, (8, 128), 1)
    keep = ((sub8 >> 1) & 1) == 0

    def lags(step, carry):
        width = 1024
        block = table_v[:, pl.ds(pl.multiple_of(step * width, width), width)]
        parts = dot(layer, block)
        hidden = sine(parts[:64] + parts[64:128] + parts[128:])
        hid_high, hid_low = split(hidden)
        twice = dot(proj_both, hid_high)
        taps = twice[:8] + twice[8:] + dot(proj_high, hid_low)
        for i in range(width // 128):
            at = step * width + i * 128 + lag8
            piece = taps[:, 128 * i : 128 * (i + 1)] * jnp.exp(decay_rows * (at.astype(F32) * (-1.0 / (LENGTH - 1))))
            piece = jnp.where(at == 0, jnp.where(keep, piece + start_rows, 0.0), piece)
            to = ((i % 2) * 32 + i // 2 + step * 4) * 8
            lag_taps[pl.ds(pl.multiple_of(to, 8), 8), :] = piece
        return carry

    lax.fori_loop(0, LENGTH // 1024, lags, 0)

    twist = (twist_v[0], twist_v[1])
    inner_in = (inner_in_v[0], inner_in_v[1])
    inner_out = (inner_out_v[0], inner_out_v[1])
    for o in range(2):
        signals = jnp.concatenate([lag_taps[pl.ds(4 * o + k, 64, stride=8), :] for k in range(4)], axis=1)
        spectra[o] = filter_spectrum(signals, outer_in_v[...], twist, inner_in)
    tables = (outer_in_v[...], outer_out_v[...], twist, inner_in, inner_out)

    lane = lax.broadcasted_iota(jnp.int32, (32, 128), 1)
    sub = lax.broadcasted_iota(jnp.int32, (32, 128), 0)

    def arrived(buffer):
        grid_v[...] = buffer[...].astype(F32).reshape(ROWS * 8, 128)

    def loaded(k, c):
        return [grid_v[pl.ds(4 * k + 2 * c + h, 32, stride=8), :] for h in range(2)]

    def short(k, role):
        whole = []
        for c in range(2):
            here = loaded(k, c)
            before, after = shifted(here, lane, sub)
            weight = [own_taps[c][j, role : role + 1] for j in range(3)]
            whole.append(
                jnp.concatenate(
                    [before[h] * weight[0] + here[h] * weight[1] + after[h] * weight[2] for h in range(2)], axis=0
                )
            )
        return jnp.concatenate(whole, axis=1)

    row_peers(lambda r: from_row(*first_trip, r).wait_recv())
    arrived(recv1)
    value = short(0, 0)
    first = short(1, 1)
    inner = first * convolve(value, spectra[0], tables)
    second_conv = convolve(inner, spectra[1], tables)

    row_peers(lambda r: from_row(*second_trip, r).wait_recv())
    arrived(recv2)
    second = short(0, 2)
    gate = jnp.concatenate([jnp.concatenate(loaded(1, c), axis=0) for c in range(2)], axis=1)
    outer = second * second_conv * (gate / (1.0 + jnp.exp(-gate)))

    for c in range(2):
        for h in range(2):
            back_v[pl.ds(2 * c + h, 32, stride=8), :] = outer[32 * h : 32 * (h + 1), 128 * c : 128 * (c + 1)]
    for r in range(ROWS):
        send3[r] = back_v[8 * r : 8 * r + 4, :].astype(BF16)
    recv3[pl.ds(row, 1)] = send3[pl.ds(row, 1)]
    row_peers(lambda r: to_row(*back_trip, r).start())

    col_peers(lambda c: weights_from(c).wait_recv())
    swap = pltpu.make_async_remote_copy(
        src_ref=w_full.at[core], dst_ref=w_full.at[core], send_sem=swap_send, recv_sem=swap_recv,
        device_id=(partner, col), device_id_type=MESH,
    )
    swap.start()

    row_peers(lambda r: from_row(*back_trip, r).wait_recv())
    for r in range(ROWS):
        block_v[4 * r : 4 * r + 4, :] = recv3[r].astype(F32)
    flipped = jnp.transpose(block_v[...]).astype(BF16)
    i128 = lax.broadcasted_iota(jnp.int32, (128, 256), 0)
    l256 = lax.broadcasted_iota(jnp.int32, (128, 256), 1)
    spread = jnp.where(l256 == 128 * (i128 & 1) + 64 * lax.rem(col, 2) + (i128 >> 1), 1.0, 0.0).astype(BF16)
    rows = dot(flipped, spread).astype(BF16)
    for h in range(2):
        send4[8 * h : 8 * (h + 1)] = rows[:, 128 * h : 128 * (h + 1)].reshape(8, 16, 128)
    recv4[pl.ds(col, 1)] = send4[pl.ds(col, 1)]
    col_peers(lambda c: to_col(*last_trip, c).start())

    swap.wait()
    col_peers(lambda c: from_col(*last_trip, c).wait_recv())
    left = jnp.concatenate([recv4[2 * m] + recv4[2 * m + 1] for m in range(8)], axis=1)
    for k in range(2):
        out_ref[0, :, 1024 * k : 1024 * (k + 1)] = dot(left, w_full[k]).astype(BF16)

    row_peers(lambda r: to_row(*first_trip, r).wait_send())
    row_peers(lambda r: to_row(*second_trip, r).wait_send())
    row_peers(lambda r: to_row(*back_trip, r).wait_send())
    col_peers(lambda c: to_col(*last_trip, c).wait_send())
    col_peers(lambda c: weights_to(c).wait_send())


def body(
    tokens, w_value, w_first, w_second, w_gate, conv_taps, filter_embed, filter_freq, filter_proj, filter_decay,
    skip_gain, w_out,
):
    consts = [jnp.asarray(c) for c in constants()]
    vmem = pltpu.VMEM
    sem = pltpu.SemaphoreType.DMA
    scratch = [
        vmem((256, 2048), BF16),
        vmem((4, 2048, 64), BF16),
        vmem((3, 3, 64), F32),
        vmem((FEATS, 64), F32),
        vmem((1, 64), F32),
        vmem((64, 2, 2, 64), F32),
        vmem((2, 2, 64), F32),
        vmem((2, 64), F32),
        vmem((128, 192), BF16),
        vmem((64, 384), BF16),
        vmem((2, 64, 128), F32),
        vmem((2, 256, 256), BF16),
        vmem((2, 256, 256), BF16),
        vmem((128, LENGTH), BF16),
        vmem((2, 1024, 1024), BF16),
        vmem((3, 128, 128), F32),
        vmem((512, 128), F32),
        vmem((2, 128, 256), F32),
        vmem((256, 128), F32),
        vmem((ROWS, 8, 128), BF16),
        vmem((ROWS, 8, 128), BF16),
        vmem((ROWS, 8, 128), BF16),
        vmem((ROWS, 8, 128), BF16),
        vmem((256, 128), F32),
        vmem((ROWS, 4, 128), BF16),
        vmem((ROWS, 4, 128), BF16),
        vmem((128, 128), F32),
        vmem((COLS, 16, 128), BF16),
        vmem((COLS, 16, 128), BF16),
        sem((18,)),
        sem((ROWS,)), sem((ROWS,)), sem((ROWS,)), sem((ROWS,)), sem((ROWS,)), sem((ROWS,)),
        sem((COLS,)), sem((COLS,)), sem((COLS,)), sem((COLS,)),
        sem, sem,
    ]
    anywhere = pl.BlockSpec(memory_space=pl.ANY)
    return pl.pallas_call(
        kernel,
        out_shape=jax.ShapeDtypeStruct((1, 16, 2048), BF16),
        in_specs=[anywhere] * 18,
        out_specs=pl.BlockSpec(memory_space=pltpu.VMEM),
        scratch_shapes=scratch,
        compiler_params=pltpu.CompilerParams(
            collective_id=0, has_side_effects=True, vmem_limit_bytes=48 * 1024 * 1024
        ),
    )(
        tokens, w_value, w_first, w_second, w_gate, conv_taps, filter_embed, filter_freq.reshape(1, -1),
        filter_proj, filter_decay, skip_gain, w_out, *consts,
    )


def solution(mesh):
    placed = (
        P(None, "row", None),
        P(None, "col"),
        P(None, "col"),
        P(None, "col"),
        P(None, "col"),
        P(None, None, "col"),
        P(),
        P(),
        P(None, None, None, "col"),
        P(None, None, "col"),
        P(None, "col"),
        P("col", None),
    )
    return jax.shard_map(
        body, mesh=mesh, in_specs=placed, out_specs=P(None, ("row", "col"), None), check_vma=False
    )
```

```python
import functools
import math

import jax
import jax.numpy as jnp
import ml_dtypes
import numpy as np
from jax import lax
from jax.experimental import pallas as pl
from jax.experimental.pallas import tpu as pltpu
from jax.sharding import PartitionSpec as P

MESH = pl.DeviceIdType.MESH
F32 = jnp.float32
BF16 = jnp.bfloat16

LENGTH = 8192
ROWS = 32
COLS = 16
FEATS = 33
FEAT_STEP = 40


def halves(x):
    x = np.asarray(x, np.float64)
    high = x.astype(ml_dtypes.bfloat16)
    low = (x - high.astype(np.float64)).astype(ml_dtypes.bfloat16)
    return high, low


@functools.lru_cache(None)
def constants():
    two_pi = 2.0 * math.pi
    j = np.arange(64)
    q = 2 * (j % 32) + j // 32
    k1 = np.arange(64) + 0.5
    p = np.arange(128)
    first = np.concatenate([np.cos(two_pi * np.outer(k1, q) / 128), -np.sin(two_pi * np.outer(k1, q) / 128)], axis=0)
    f_high, f_low = halves(first)
    outer_in = np.concatenate([f_high, f_high, f_low], axis=1)
    outer_out = np.concatenate([f_high.T, f_high.T, f_low.T], axis=1)
    twist = np.stack(
        [np.cos(two_pi * np.outer(k1, p) / 16384), -np.sin(two_pi * np.outer(k1, p) / 16384)]
    ).astype(np.float32)
    g_real = np.cos(two_pi * (np.outer(p, p) % 128) / 128)
    g_imag = -np.sin(two_pi * (np.outer(p, p) % 128) / 128)
    inner_in = np.stack(halves(np.block([[g_real, g_imag], [-g_imag, g_real]])))
    inner_out = np.stack(halves(np.block([[g_real, -g_imag], [g_imag, g_real]])))
    n = np.arange(LENGTH)
    b = np.arange(1, 17)
    phase = two_pi * (np.outer(b, n) % LENGTH) / LENGTH
    features = np.concatenate([(n / (LENGTH - 1))[None], np.cos(phase), np.sin(phase)], axis=0)
    table = np.zeros((128, LENGTH), ml_dtypes.bfloat16)
    rest = features
    for part in range(3):
        piece = rest.astype(ml_dtypes.bfloat16)
        table[part * FEAT_STEP : part * FEAT_STEP + FEATS] = piece
        rest = rest - piece.astype(np.float64)
    return outer_in, outer_out, twist, inner_in, inner_out, table


def split(x):
    high = x.astype(BF16)
    return high, (x - high.astype(F32)).astype(BF16)


def dot(a, b):
    return jnp.dot(a, b, preferred_element_type=F32)


def dot_nt(a, b, precision=None):
    return lax.dot_general(a, b, (((1,), (1,)), ((), ())), precision=precision, preferred_element_type=F32)


def times(x, matrix):
    high, low = split(x)
    return dot(high, matrix[0]) + dot(low, matrix[0]) + dot(high, matrix[1])


def forward(signal, outer_in, twist, inner_in):
    high, low = split(signal)
    stage = dot(outer_in, jnp.concatenate([high, low, high], axis=0))
    turned = []
    for m in range(signal.shape[1] // 128):
        real = stage[:64, 128 * m : 128 * (m + 1)]
        imag = stage[64:, 128 * m : 128 * (m + 1)]
        turned.append(
            jnp.concatenate([real * twist[0] - imag * twist[1], real * twist[1] + imag * twist[0]], axis=1)
        )
    return times(jnp.concatenate(turned, axis=0), inner_in)


def inverse(spectrum, outer_out, twist, inner_out):
    stage = times(spectrum, inner_out)
    reals, imags = [], []
    for m in range(spectrum.shape[0] // 64):
        real = stage[64 * m : 64 * (m + 1), :128]
        imag = stage[64 * m : 64 * (m + 1), 128:]
        reals.append(real * twist[0] + imag * twist[1])
        imags.append(imag * twist[0] - real * twist[1])
    both = jnp.concatenate([jnp.concatenate(reals, axis=1), jnp.concatenate(imags, axis=1)], axis=0)
    high, low = split(both)
    return dot(outer_out, jnp.concatenate([high, low, high], axis=0))


def convolve(signal, filt, tables):
    outer_in, outer_out, twist, inner_in, inner_out = tables
    spectrum = forward(signal, outer_in, twist, inner_in)
    real, imag = spectrum[:, :128], spectrum[:, 128:]
    f_real, f_imag = filt[:, :128], filt[:, 128:]
    product = jnp.concatenate([real * f_real - imag * f_imag, real * f_imag + imag * f_real], axis=1)
    return inverse(product, outer_out, twist, inner_out)


def filter_spectrum(signals, outer_in, twist, inner_in):
    spectra = forward(signals, outer_in, twist, inner_in)
    ahead, behind = spectra[:128], spectra[128:]
    scale = 2.0 / (2 * LENGTH)
    return jnp.concatenate(
        [(ahead[:, :128] + behind[:, :128]) * scale, (ahead[:, 128:] - behind[:, 128:]) * scale], axis=1
    )


def sine(x):
    k = jnp.floor(x * (1.0 / math.pi) + 0.5)
    r = x - k * 3.140625
    r = r - k * 9.67502593994140625e-4
    r = r - k * 1.509957990978376432e-7
    half = k * 0.5
    sign = 1.0 - 4.0 * (half - jnp.floor(half))
    s = r * r
    poly = -1.0 / 39916800.0
    for c in (1.0 / 362880.0, -1.0 / 5040.0, 1.0 / 120.0, -1.0 / 6.0):
        poly = poly * s + c
    return sign * (r + r * (s * poly))


def shifted(parts, lane, sub):
    right = [pltpu.roll(x, 1, 1) for x in parts]
    left = [pltpu.roll(x, 127, 1) for x in parts]
    carry = jnp.where(sub == 0, 0.0, pltpu.roll(right[1], 1, 0))
    back = jnp.where(sub == 31, 0.0, pltpu.roll(left[0], 31, 0))
    before = [jnp.where(lane == 0, carry, right[0]), jnp.where(lane == 0, right[0], right[1])]
    after = [jnp.where(lane == 127, left[1], left[0]), jnp.where(lane == 127, back, left[1])]
    return before, after


def kernel(
    tokens, w_value, w_first, w_second, w_gate, conv_taps, embed, freq, proj, decay, gain, w_out,
    outer_in_h, outer_out_h, twist_h, inner_in_h, inner_out_h, table_h,
    out_ref,
    tok_v, w_v, taps_v, embed_v, freq_v, proj_v, decay_v, gain_v,
    outer_in_v, outer_out_v, twist_v, inner_in_v, inner_out_v, table_v,
    w_full, est, lag_taps, spectra, grid_v, send1, recv1, send2, recv2, back_v, send3, recv3, block_v, send4, recv4,
    load_sem, send_sem1, recv_sem1, send_sem2, recv_sem2, send_sem3, recv_sem3, send_sem4, recv_sem4,
    send_sem5, recv_sem5, swap_send, swap_recv,
):
    row = lax.axis_index("row")
    col = lax.axis_index("col")
    z = lax.div(row, 2)
    core = lax.rem(row, 2)
    partner = z * 2 + 1 - core
    y = lax.div(col, 4)
    x = lax.rem(col, 4)

    def row_peers(visit):
        def step(i, carry):
            away = 8 + lax.div(i + 1, 2) * (1 - 2 * lax.rem(i, 2))
            there = lax.rem(z + away, 16) * 2
            visit(there)
            visit(there + 1)
            return carry

        lax.fori_loop(0, 15, step, 0)
        visit(partner)

    def col_peers(visit):
        def step(i, carry):
            visit(lax.rem(col + i, COLS))
            return carry

        lax.fori_loop(1, COLS, step, 0)

    barrier = pltpu.get_barrier_semaphore()
    row_peers(lambda r: pl.semaphore_signal(barrier, inc=1, device_id=(r, col), device_id_type=MESH))
    col_peers(lambda c: pl.semaphore_signal(barrier, inc=1, device_id=(row, c), device_id_type=MESH))

    loads = []
    for source, target in (
        (tokens.at[0], tok_v),
        (w_value, w_v.at[pl.ds(0, 64)]),
        (w_first, w_v.at[pl.ds(64, 64)]),
        (w_second, w_v.at[pl.ds(128, 64)]),
        (w_gate, w_v.at[pl.ds(192, 64)]),
        (w_out.at[:, pl.ds(pl.multiple_of(core * 1024, 512), 512)], w_full.at[core, 0, y, x]),
        (w_out.at[:, pl.ds(pl.multiple_of(core * 1024 + 512, 512), 512)], w_full.at[core, 1, y, x]),
        (conv_taps, taps_v),
        (embed, embed_v),
        (freq, freq_v),
        (proj, proj_v),
        (decay, decay_v),
        (gain, gain_v),
        (table_h, table_v),
        (outer_in_h, outer_in_v),
        (outer_out_h, outer_out_v),
        (twist_h, twist_v),
        (inner_in_h, inner_in_v),
        (inner_out_h, inner_out_v),
    ):
        load = pltpu.make_async_copy(source, target, load_sem.at[len(loads)])
        load.start()
        loads.append(load)

    for load in loads[:5]:
        load.wait()
    result = dot_nt(w_v[...], tok_v[...]).astype(BF16)
    order = lax.broadcasted_iota(jnp.int32, (256, 256), 0)
    source = lax.broadcasted_iota(jnp.int32, (256, 256), 1)
    match = ((order >> 2) & 1) * 128 + (order & 1) * 64 + 2 * (order >> 3) + ((order >> 1) & 1)
    place = jnp.where(source == match, 1.0, 0.0).astype(BF16)
    parts = [
        jnp.concatenate(
            [result[64 * k : 64 * (k + 1), 128 * h : 128 * (h + 1)] for k in (pair, pair + 1) for h in range(2)], axis=0
        )
        for pair in (0, 2)
    ]
    sorted_rows = dot(place, jnp.concatenate(parts, axis=1))
    send1[...] = sorted_rows[:, :128].reshape(ROWS, 8, 128).astype(BF16)
    send2[...] = sorted_rows[:, 128:].reshape(ROWS, 8, 128).astype(BF16)
    recv1[pl.ds(row, 1)] = send1[pl.ds(row, 1)]
    recv2[pl.ds(row, 1)] = send2[pl.ds(row, 1)]
    loads[5].wait()
    loads[6].wait()

    def to_row(source, target, sent, received, r):
        return pltpu.make_async_remote_copy(
            src_ref=source.at[r], dst_ref=target.at[row], send_sem=sent.at[r], recv_sem=received.at[row],
            device_id=(r, col), device_id_type=MESH,
        )

    def from_row(source, target, sent, received, r):
        return pltpu.make_async_remote_copy(
            src_ref=source.at[r], dst_ref=target.at[r], send_sem=sent.at[r], recv_sem=received.at[r],
            device_id=(r, col), device_id_type=MESH,
        )

    def to_col(source, target, sent, received, c):
        return pltpu.make_async_remote_copy(
            src_ref=source.at[c], dst_ref=target.at[col], send_sem=sent.at[c], recv_sem=received.at[col],
            device_id=(row, c), device_id_type=MESH,
        )

    def from_col(source, target, sent, received, c):
        return pltpu.make_async_remote_copy(
            src_ref=source.at[c], dst_ref=target.at[c], send_sem=sent.at[c], recv_sem=received.at[c],
            device_id=(row, c), device_id_type=MESH,
        )

    def along_x(i):
        return lax.rem(x + i, 4)

    def along_y(i):
        return lax.rem(y + i, 4)

    def gather(leg, part, i, sending):
        by_x = leg == part
        other = along_x(i) if by_x else along_y(i)
        device = y * 4 + other if by_x else other * 4 + x
        if leg == 0:
            here, there = w_full.at[core, part, y, x], w_full.at[core, part, y if by_x else other, other if by_x else x]
        elif by_x:
            here, there = w_full.at[core, part, :, x], w_full.at[core, part, :, other]
        else:
            here, there = w_full.at[core, part, y], w_full.at[core, part, other]
        slot = 2 * leg + part
        return pltpu.make_async_remote_copy(
            src_ref=here, dst_ref=here if sending else there, send_sem=send_sem5.at[slot, other],
            recv_sem=recv_sem5.at[slot, (x if by_x else y) if sending else other],
            device_id=(row, device), device_id_type=MESH,
        )

    def gather_all(leg, visit):
        for part in range(2):
            for i in (2, 1, 3):
                visit(part, i)

    first_trip = (send1, recv1, send_sem1, recv_sem1)
    second_trip = (send2, recv2, send_sem2, recv_sem2)
    back_trip = (send3, recv3, send_sem3, recv_sem3)
    last_trip = (send4, recv4, send_sem4, recv_sem4)

    pl.semaphore_wait(barrier, ROWS - 1 + COLS - 1)
    row_peers(lambda r: to_row(*first_trip, r).start())
    row_peers(lambda r: to_row(*second_trip, r).start())
    gather_all(0, lambda part, i: gather(0, part, i, True).start())

    for load in loads[7:]:
        load.wait()
    scaled = embed_v[...] * freq_v[...]
    est[...] = jnp.zeros_like(est)
    high = scaled.astype(BF16).astype(F32)
    rest = scaled - high
    mid = rest.astype(BF16).astype(F32)
    low = rest - mid
    for k, parts in enumerate(((high, high, high), (mid, mid), (low,))):
        for m, part in enumerate(parts):
            est[k, FEAT_STEP * m : FEAT_STEP * m + FEATS, :64] = part
    layer = jnp.concatenate([jnp.transpose(est[k])[:64] for k in range(3)], axis=0).astype(BF16)

    lane64 = lax.broadcasted_iota(jnp.int32, (8, 64), 1)
    sub64 = lax.broadcasted_iota(jnp.int32, (8, 64), 0)
    own_proj = jnp.zeros((8, 64), F32)
    for o in range(2):
        for d in range(2):
            pick = jnp.where((lane64 == 2 * row + (sub64 & 1)) & ((sub64 >> 1) == 2 * o + d), 1.0, 0.0)
            own_proj = own_proj + dot_nt(pick, proj_v[:, o, d, :], lax.Precision.HIGHEST)
    proj_high, proj_low = split(own_proj)
    proj_both = jnp.concatenate([own_proj, own_proj - proj_high.astype(F32)], axis=0).astype(BF16)

    def own(ref):
        lanes = lax.broadcasted_iota(jnp.int32, ref.shape, len(ref.shape) - 1)
        return [jnp.sum(jnp.where(lanes == 2 * row + c, ref[...], 0.0), axis=-1, keepdims=True) for c in range(2)]

    own_taps = own(taps_v)
    own_decay = own(decay_v)
    own_gain = own(gain_v)
    sub8 = lax.broadcasted_iota(jnp.int32, (8, 128), 0)
    decay_rows = jnp.zeros((8, 128), F32)
    start_rows = jnp.zeros((8, 128), F32)
    for o in range(2):
        for c in range(2):
            start_rows = jnp.where(sub8 == 4 * o + c, own_gain[c][o : o + 1], start_rows)
            for d in range(2):
                decay_rows = jnp.where(sub8 == 4 * o + 2 * d + c, own_decay[c][o, d : d + 1], decay_rows)
    lag8 = lax.broadcasted_iota(jnp.int32, (8, 128), 1)
    keep = ((sub8 >> 1) & 1) == 0

    def lags(step, carry):
        width = 1024
        block = table_v[:, pl.ds(pl.multiple_of(step * width, width), width)]
        parts = dot(layer, block)
        hidden = sine(parts[:64] + parts[64:128] + parts[128:])
        hid_high, hid_low = split(hidden)
        twice = dot(proj_both, hid_high)
        taps = twice[:8] + twice[8:] + dot(proj_high, hid_low)
        for i in range(width // 128):
            at = step * width + i * 128 + lag8
            piece = taps[:, 128 * i : 128 * (i + 1)] * jnp.exp(decay_rows * (at.astype(F32) * (-1.0 / (LENGTH - 1))))
            piece = jnp.where(at == 0, jnp.where(keep, piece + start_rows, 0.0), piece)
            to = ((i % 2) * 32 + i // 2 + step * 4) * 8
            lag_taps[pl.ds(pl.multiple_of(to, 8), 8), :] = piece
        return carry

    lax.fori_loop(0, LENGTH // 1024, lags, 0)

    twist = (twist_v[0], twist_v[1])
    inner_in = (inner_in_v[0], inner_in_v[1])
    inner_out = (inner_out_v[0], inner_out_v[1])
    for o in range(2):
        signals = jnp.concatenate([lag_taps[pl.ds(4 * o + k, 64, stride=8), :] for k in range(4)], axis=1)
        spectra[o] = filter_spectrum(signals, outer_in_v[...], twist, inner_in)
    tables = (outer_in_v[...], outer_out_v[...], twist, inner_in, inner_out)

    lane = lax.broadcasted_iota(jnp.int32, (32, 128), 1)
    sub = lax.broadcasted_iota(jnp.int32, (32, 128), 0)

    def arrived(buffer):
        grid_v[...] = buffer[...].astype(F32).reshape(ROWS * 8, 128)

    def loaded(k, c):
        return [grid_v[pl.ds(4 * k + 2 * c + h, 32, stride=8), :] for h in range(2)]

    def short(k, role):
        whole = []
        for c in range(2):
            here = loaded(k, c)
            before, after = shifted(here, lane, sub)
            weight = [own_taps[c][j, role : role + 1] for j in range(3)]
            whole.append(
                jnp.concatenate(
                    [before[h] * weight[0] + here[h] * weight[1] + after[h] * weight[2] for h in range(2)], axis=0
                )
            )
        return jnp.concatenate(whole, axis=1)

    gather_all(0, lambda part, i: gather(0, part, i, False).wait_recv())
    gather_all(1, lambda part, i: gather(1, part, i, True).start())

    row_peers(lambda r: from_row(*first_trip, r).wait_recv())
    arrived(recv1)
    value = short(0, 0)
    first = short(1, 1)
    inner = first * convolve(value, spectra[0], tables)
    second_conv = convolve(inner, spectra[1], tables)

    row_peers(lambda r: from_row(*second_trip, r).wait_recv())
    arrived(recv2)
    second = short(0, 2)
    gate = jnp.concatenate([jnp.concatenate(loaded(1, c), axis=0) for c in range(2)], axis=1)
    outer = second * second_conv * (gate / (1.0 + jnp.exp(-gate)))

    for c in range(2):
        for h in range(2):
            back_v[pl.ds(2 * c + h, 32, stride=8), :] = outer[32 * h : 32 * (h + 1), 128 * c : 128 * (c + 1)]
    for r in range(ROWS):
        send3[r] = back_v[8 * r : 8 * r + 4, :].astype(BF16)
    recv3[pl.ds(row, 1)] = send3[pl.ds(row, 1)]
    row_peers(lambda r: to_row(*back_trip, r).start())

    gather_all(1, lambda part, i: gather(1, part, i, False).wait_recv())
    swap = pltpu.make_async_remote_copy(
        src_ref=w_full.at[core], dst_ref=w_full.at[core], send_sem=swap_send, recv_sem=swap_recv,
        device_id=(partner, col), device_id_type=MESH,
    )
    swap.start()

    row_peers(lambda r: from_row(*back_trip, r).wait_recv())
    for r in range(ROWS):
        block_v[4 * r : 4 * r + 4, :] = recv3[r].astype(F32)
    flipped = jnp.transpose(block_v[...]).astype(BF16)
    i128 = lax.broadcasted_iota(jnp.int32, (128, 256), 0)
    l256 = lax.broadcasted_iota(jnp.int32, (128, 256), 1)
    spread = jnp.where(l256 == 128 * (i128 & 1) + 64 * lax.rem(col, 2) + (i128 >> 1), 1.0, 0.0).astype(BF16)
    rows = dot(flipped, spread).astype(BF16)
    for h in range(2):
        send4[8 * h : 8 * (h + 1)] = rows[:, 128 * h : 128 * (h + 1)].reshape(8, 16, 128)
    recv4[pl.ds(col, 1)] = send4[pl.ds(col, 1)]
    col_peers(lambda c: to_col(*last_trip, c).start())

    swap.wait()
    col_peers(lambda c: from_col(*last_trip, c).wait_recv())
    left = jnp.concatenate([recv4[2 * m] + recv4[2 * m + 1] for m in range(8)], axis=1)
    for k in range(2):
        for part in range(2):
            at = 1024 * k + 512 * part
            out_ref[0, :, at : at + 512] = dot(left, w_full[k, part].reshape(1024, 512)).astype(BF16)

    row_peers(lambda r: to_row(*first_trip, r).wait_send())
    row_peers(lambda r: to_row(*second_trip, r).wait_send())
    row_peers(lambda r: to_row(*back_trip, r).wait_send())
    col_peers(lambda c: to_col(*last_trip, c).wait_send())
    gather_all(0, lambda part, i: gather(0, part, i, True).wait_send())
    gather_all(1, lambda part, i: gather(1, part, i, True).wait_send())


def body(
    tokens, w_value, w_first, w_second, w_gate, conv_taps, filter_embed, filter_freq, filter_proj, filter_decay,
    skip_gain, w_out,
):
    consts = [jnp.asarray(c) for c in constants()]
    vmem = pltpu.VMEM
    sem = pltpu.SemaphoreType.DMA
    scratch = [
        vmem((256, 2048), BF16),
        vmem((256, 2048), BF16),
        vmem((3, 3, 64), F32),
        vmem((FEATS, 64), F32),
        vmem((1, 64), F32),
        vmem((64, 2, 2, 64), F32),
        vmem((2, 2, 64), F32),
        vmem((2, 64), F32),
        vmem((128, 192), BF16),
        vmem((64, 384), BF16),
        vmem((2, 64, 128), F32),
        vmem((2, 256, 256), BF16),
        vmem((2, 256, 256), BF16),
        vmem((128, LENGTH), BF16),
        vmem((2, 2, 4, 4, 64, 512), BF16),
        vmem((3, 128, 128), F32),
        vmem((512, 128), F32),
        vmem((2, 128, 256), F32),
        vmem((256, 128), F32),
        vmem((ROWS, 8, 128), BF16),
        vmem((ROWS, 8, 128), BF16),
        vmem((ROWS, 8, 128), BF16),
        vmem((ROWS, 8, 128), BF16),
        vmem((256, 128), F32),
        vmem((ROWS, 4, 128), BF16),
        vmem((ROWS, 4, 128), BF16),
        vmem((128, 128), F32),
        vmem((COLS, 16, 128), BF16),
        vmem((COLS, 16, 128), BF16),
        sem((19,)),
        sem((ROWS,)), sem((ROWS,)), sem((ROWS,)), sem((ROWS,)), sem((ROWS,)), sem((ROWS,)),
        sem((COLS,)), sem((COLS,)), sem((4, 4)), sem((4, 4)),
        sem, sem,
    ]
    anywhere = pl.BlockSpec(memory_space=pltpu.HBM)
    return pl.pallas_call(
        kernel,
        out_shape=jax.ShapeDtypeStruct((1, 16, 2048), BF16),
        in_specs=[anywhere] * 18,
        out_specs=pl.BlockSpec(memory_space=pltpu.VMEM),
        scratch_shapes=scratch,
        compiler_params=pltpu.CompilerParams(
            collective_id=0, has_side_effects=True, vmem_limit_bytes=67043328
        ),
    )(
        tokens, w_value.T, w_first.T, w_second.T, w_gate.T, conv_taps, filter_embed, filter_freq.reshape(1, -1),
        filter_proj, filter_decay, skip_gain, w_out, *consts,
    )


def solution(mesh):
    placed = (
        P(None, "row", None),
        P(None, "col"),
        P(None, "col"),
        P(None, "col"),
        P(None, "col"),
        P(None, None, "col"),
        P(),
        P(),
        P(None, None, None, "col"),
        P(None, None, "col"),
        P(None, "col"),
        P("col", None),
    )
    return jax.shard_map(
        body, mesh=mesh, in_specs=placed, out_specs=P(None, ("row", "col"), None), check_vma=False
    )
```

```python
import functools
import math

import jax
import jax.numpy as jnp
import ml_dtypes
import numpy as np
from jax import lax
from jax.experimental import pallas as pl
from jax.experimental.pallas import tpu as pltpu
from jax.sharding import PartitionSpec as P

MESH = pl.DeviceIdType.MESH
F32 = jnp.float32
BF16 = jnp.bfloat16

LENGTH = 8192
ROWS = 32
COLS = 16
FEATS = 33
FEAT_STEP = 40


def halves(x):
    x = np.asarray(x, np.float64)
    high = x.astype(ml_dtypes.bfloat16)
    low = (x - high.astype(np.float64)).astype(ml_dtypes.bfloat16)
    return high, low


@functools.lru_cache(None)
def constants():
    two_pi = 2.0 * math.pi
    j = np.arange(64)
    q = 2 * (j % 32) + j // 32
    k1 = np.arange(64) + 0.5
    p = np.arange(128)
    first = np.concatenate([np.cos(two_pi * np.outer(k1, q) / 128), -np.sin(two_pi * np.outer(k1, q) / 128)], axis=0)
    f_high, f_low = halves(first)
    outer_in = np.concatenate([f_high, f_high, f_low], axis=1)
    outer_out = np.concatenate([f_high.T, f_high.T, f_low.T], axis=1)
    twist = np.stack(
        [np.cos(two_pi * np.outer(k1, p) / 16384), -np.sin(two_pi * np.outer(k1, p) / 16384)]
    ).astype(np.float32)
    g_real = np.cos(two_pi * (np.outer(p, p) % 128) / 128)
    g_imag = -np.sin(two_pi * (np.outer(p, p) % 128) / 128)
    inner_in = np.stack(halves(np.block([[g_real, g_imag], [-g_imag, g_real]])))
    inner_out = np.stack(halves(np.block([[g_real, -g_imag], [g_imag, g_real]])))
    n = np.arange(LENGTH)
    b = np.arange(1, 17)
    phase = two_pi * (np.outer(b, n) % LENGTH) / LENGTH
    features = np.concatenate([(n / (LENGTH - 1))[None], np.cos(phase), np.sin(phase)], axis=0)
    table = np.zeros((128, LENGTH), ml_dtypes.bfloat16)
    rest = features
    for part in range(3):
        piece = rest.astype(ml_dtypes.bfloat16)
        table[part * FEAT_STEP : part * FEAT_STEP + FEATS] = piece
        rest = rest - piece.astype(np.float64)
    return outer_in, outer_out, twist, inner_in, inner_out, table


def split(x):
    high = x.astype(BF16)
    return high, (x - high.astype(F32)).astype(BF16)


def dot(a, b):
    return jnp.dot(a, b, preferred_element_type=F32)


def dot_nt(a, b, precision=None):
    return lax.dot_general(a, b, (((1,), (1,)), ((), ())), precision=precision, preferred_element_type=F32)


def times(x, matrix):
    high, low = split(x)
    return dot(high, matrix[0]) + dot(low, matrix[0]) + dot(high, matrix[1])


def forward(signal, outer_in, twist, inner_in):
    high, low = split(signal)
    stage = dot(outer_in, jnp.concatenate([high, low, high], axis=0))
    turned = []
    for m in range(signal.shape[1] // 128):
        real = stage[:64, 128 * m : 128 * (m + 1)]
        imag = stage[64:, 128 * m : 128 * (m + 1)]
        turned.append(
            jnp.concatenate([real * twist[0] - imag * twist[1], real * twist[1] + imag * twist[0]], axis=1)
        )
    return times(jnp.concatenate(turned, axis=0), inner_in)


def inverse(spectrum, outer_out, twist, inner_out):
    stage = times(spectrum, inner_out)
    reals, imags = [], []
    for m in range(spectrum.shape[0] // 64):
        real = stage[64 * m : 64 * (m + 1), :128]
        imag = stage[64 * m : 64 * (m + 1), 128:]
        reals.append(real * twist[0] + imag * twist[1])
        imags.append(imag * twist[0] - real * twist[1])
    both = jnp.concatenate([jnp.concatenate(reals, axis=1), jnp.concatenate(imags, axis=1)], axis=0)
    high, low = split(both)
    return dot(outer_out, jnp.concatenate([high, low, high], axis=0))


def convolve(signal, filt, tables):
    outer_in, outer_out, twist, inner_in, inner_out = tables
    spectrum = forward(signal, outer_in, twist, inner_in)
    real, imag = spectrum[:, :128], spectrum[:, 128:]
    f_real, f_imag = filt[:, :128], filt[:, 128:]
    product = jnp.concatenate([real * f_real - imag * f_imag, real * f_imag + imag * f_real], axis=1)
    return inverse(product, outer_out, twist, inner_out)


def filter_spectrum(signals, outer_in, twist, inner_in):
    spectra = forward(signals, outer_in, twist, inner_in)
    ahead, behind = spectra[:128], spectra[128:]
    scale = 2.0 / (2 * LENGTH)
    return jnp.concatenate(
        [(ahead[:, :128] + behind[:, :128]) * scale, (ahead[:, 128:] - behind[:, 128:]) * scale], axis=1
    )


def sine(x):
    k = jnp.floor(x * (1.0 / math.pi) + 0.5)
    r = x - k * 3.140625
    r = r - k * 9.67502593994140625e-4
    r = r - k * 1.509957990978376432e-7
    half = k * 0.5
    sign = 1.0 - 4.0 * (half - jnp.floor(half))
    s = r * r
    poly = -1.0 / 39916800.0
    for c in (1.0 / 362880.0, -1.0 / 5040.0, 1.0 / 120.0, -1.0 / 6.0):
        poly = poly * s + c
    return sign * (r + r * (s * poly))


def shifted(parts, lane, sub):
    right = [pltpu.roll(x, 1, 1) for x in parts]
    left = [pltpu.roll(x, 127, 1) for x in parts]
    carry = jnp.where(sub == 0, 0.0, pltpu.roll(right[1], 1, 0))
    back = jnp.where(sub == 31, 0.0, pltpu.roll(left[0], 31, 0))
    before = [jnp.where(lane == 0, carry, right[0]), jnp.where(lane == 0, right[0], right[1])]
    after = [jnp.where(lane == 127, left[1], left[0]), jnp.where(lane == 127, back, left[1])]
    return before, after


def kernel(
    tokens, w_value, w_first, w_second, w_gate, conv_taps, embed, freq, proj, decay, gain, w_out,
    outer_in_h, outer_out_h, twist_h, inner_in_h, inner_out_h, table_h,
    out_ref,
    tok_v, w_v, taps_v, embed_v, freq_v, proj_v, decay_v, gain_v,
    outer_in_v, outer_out_v, twist_v, inner_in_v, inner_out_v, table_v,
    w_full, est, lag_taps, spectra, sort_v, gate_v, block_v, back_v, edge_out, edge_in,
    send1, recv1, send2, recv2, send3, recv3, send4, recv4,
    load_sem, send_sem1, recv_sem1, send_sem2, recv_sem2, send_sem3, recv_sem3, send_sem4, recv_sem4,
    edge_send, edge_recv, block_send, block_recv, hop_send, hop_recv, swap_send, swap_recv,
):
    row = lax.axis_index("row")
    col = lax.axis_index("col")
    z = lax.div(row, 2)
    core = lax.rem(row, 2)
    partner = z * 2 + 1 - core
    y = lax.div(col, 4)
    x = lax.rem(col, 4)

    def row_peers(visit):
        def step(i, carry):
            away = 8 + lax.div(i + 1, 2) * (1 - 2 * lax.rem(i, 2))
            there = lax.rem(z + away, 16) * 2
            visit(there)
            visit(there + 1)
            return carry

        lax.fori_loop(0, 15, step, 0)
        visit(partner)

    def col_peers(visit):
        def step(i, carry):
            visit(lax.rem(col + i, COLS))
            return carry

        lax.fori_loop(1, COLS, step, 0)

    barrier = pltpu.get_barrier_semaphore()
    row_peers(lambda r: pl.semaphore_signal(barrier, inc=1, device_id=(r, col), device_id_type=MESH))
    col_peers(lambda c: pl.semaphore_signal(barrier, inc=1, device_id=(row, c), device_id_type=MESH))

    loads = []
    for source, target in (
        (tokens.at[0], tok_v),
        (w_value, w_v.at[pl.ds(0, 64)]),
        (w_first, w_v.at[pl.ds(64, 64)]),
        (w_second, w_v.at[pl.ds(128, 64)]),
        (w_gate, w_v.at[pl.ds(192, 64)]),
        (w_out.at[:, pl.ds(pl.multiple_of(core * 1024, 512), 512)], w_full.at[core, 0, y, x]),
        (w_out.at[:, pl.ds(pl.multiple_of(core * 1024 + 512, 512), 512)], w_full.at[core, 1, y, x]),
        (conv_taps, taps_v),
        (embed, embed_v),
        (freq, freq_v),
        (proj, proj_v),
        (decay, decay_v),
        (gain, gain_v),
        (table_h, table_v),
        (outer_in_h, outer_in_v),
        (outer_out_h, outer_out_v),
        (twist_h, twist_v),
        (inner_in_h, inner_in_v),
        (inner_out_h, inner_out_v),
    ):
        load = pltpu.make_async_copy(source, target, load_sem.at[len(loads)])
        load.start()
        loads.append(load)

    for load in loads[:5]:
        load.wait()
    result = dot_nt(w_v[...], tok_v[...]).astype(BF16)
    order = lax.broadcasted_iota(jnp.int32, (128, 128), 0)
    source = lax.broadcasted_iota(jnp.int32, (128, 128), 1)
    place = jnp.where(source == (order & 1) * 64 + (order >> 1), 1.0, 0.0).astype(BF16)
    roles = [
        jnp.concatenate([result[64 * k : 64 * (k + 1), :128], result[64 * k : 64 * (k + 1), 128:]], axis=0)
        for k in range(4)
    ]
    sort_v[...] = dot(place, jnp.concatenate(roles, axis=1))
    for r in range(ROWS):
        send1[r] = sort_v[4 * r : 4 * r + 4, :128].astype(BF16)
        send2[r] = sort_v[4 * r : 4 * r + 4, 128:256].astype(BF16)
    recv1[pl.ds(row, 1)] = send1[pl.ds(row, 1)]
    recv2[pl.ds(row, 1)] = send2[pl.ds(row, 1)]
    end_row = lax.broadcasted_iota(jnp.int32, (16, 256), 0)
    end_col = lax.broadcasted_iota(jnp.int32, (16, 256), 1)
    ends = jnp.where(end_col == 255 * end_row, 1.0, 0.0).astype(BF16)
    edge_out[...] = dot_nt(ends, result[128:]).astype(BF16)
    loads[5].wait()
    loads[6].wait()

    def to_row(trip, r):
        source, target, sent, received = trip
        return pltpu.make_async_remote_copy(
            src_ref=source.at[r], dst_ref=target.at[row], send_sem=sent, recv_sem=received,
            device_id=(r, col), device_id_type=MESH,
        )

    def to_col(trip, c):
        source, target, sent, received = trip
        return pltpu.make_async_remote_copy(
            src_ref=source.at[c], dst_ref=target.at[col], send_sem=sent, recv_sem=received,
            device_id=(row, c), device_id_type=MESH,
        )

    def whole(trip):
        source, target, sent, received = trip
        count = pl.ds(0, source.shape[0] - 1)
        return pltpu.make_async_remote_copy(
            src_ref=source.at[count], dst_ref=target.at[count], send_sem=sent, recv_sem=received,
            device_id=(partner, col), device_id_type=MESH,
        )

    def edge(step, slot):
        return pltpu.make_async_remote_copy(
            src_ref=edge_out, dst_ref=edge_in.at[slot], send_sem=edge_send.at[slot], recv_sem=edge_recv.at[slot],
            device_id=(lax.rem(row + step, ROWS), col), device_id_type=MESH,
        )

    after_me, before_me = edge(1, 0), edge(ROWS - 1, 1)

    def block(part, yy, xx):
        return w_full.at[core, part, yy, xx]

    def group(part, step, half=None):
        some = slice(None) if half is None else pl.ds(2 * half, 2)
        if part == 0:
            return w_full.at[core, 0, lax.rem(y + step, 4), some]
        return w_full.at[core, 1, some, lax.rem(x + step, 4)]

    def across(part, step):
        return lax.rem(y + step, 4) * 4 + x if part == 0 else y * 4 + lax.rem(x + step, 4)

    def spread_block(part, step):
        there = y * 4 + lax.rem(x + step, 4) if part == 0 else lax.rem(y + step, 4) * 4 + x
        return pltpu.make_async_remote_copy(
            src_ref=block(part, y, x), dst_ref=block(part, y, x), send_sem=block_send.at[part],
            recv_sem=block_recv.at[part], device_id=(row, there), device_id_type=MESH,
        )

    def blocks(part):
        three = w_full.at[core, part, 0, pl.ds(0, 3)]
        return pltpu.make_async_remote_copy(
            src_ref=three, dst_ref=three, send_sem=block_send.at[part], recv_sem=block_recv.at[part],
            device_id=(partner, col), device_id_type=MESH,
        )

    def hop(part, step, held, half=None):
        side = (0 if half is None else 2) + (0 if step == 1 else 1)
        here = group(part, held, half)
        return pltpu.make_async_remote_copy(
            src_ref=here, dst_ref=here, send_sem=hop_send.at[part, side], recv_sem=hop_recv.at[part, side],
            device_id=(row, across(part, step)), device_id_type=MESH,
        )

    def hops(half):
        if half:
            return [hop(part, step, 4 - step, 0 if step == 1 else 1) for part in range(2) for step in (1, 3)]
        return [hop(part, step, 0) for part in range(2) for step in (1, 3)]

    def swap(part, step):
        here = group(part, step)
        return pltpu.make_async_remote_copy(
            src_ref=here, dst_ref=here, send_sem=swap_send, recv_sem=swap_recv,
            device_id=(partner, col), device_id_type=MESH,
        )

    value_trip = (send1, recv1, send_sem1, recv_sem1)
    first_trip = (send2, recv2, send_sem2, recv_sem2)
    back_trip = (send3, recv3, send_sem3, recv_sem3)
    last_trip = (send4, recv4, send_sem4, recv_sem4)

    pl.semaphore_wait(barrier, ROWS - 1 + COLS - 1)
    row_peers(lambda r: to_row(value_trip, r).start())
    for part in range(2):
        for step in (2, 1, 3):
            spread_block(part, step).start()
    row_peers(lambda r: to_row(first_trip, r).start())
    after_me.start()
    before_me.start()

    for load in loads[7:]:
        load.wait()
    scaled = embed_v[...] * freq_v[...]
    est[...] = jnp.zeros_like(est)
    high = scaled.astype(BF16).astype(F32)
    rest = scaled - high
    mid = rest.astype(BF16).astype(F32)
    low = rest - mid
    for k, parts in enumerate(((high, high, high), (mid, mid), (low,))):
        for m, part in enumerate(parts):
            est[k, FEAT_STEP * m : FEAT_STEP * m + FEATS, :64] = part
    layer = jnp.concatenate([jnp.transpose(est[k])[:64] for k in range(3)], axis=0).astype(BF16)

    lane64 = lax.broadcasted_iota(jnp.int32, (8, 64), 1)
    sub64 = lax.broadcasted_iota(jnp.int32, (8, 64), 0)
    own_proj = jnp.zeros((8, 64), F32)
    for o in range(2):
        for d in range(2):
            pick = jnp.where((lane64 == 2 * row + (sub64 & 1)) & ((sub64 >> 1) == 2 * o + d), 1.0, 0.0)
            own_proj = own_proj + dot_nt(pick, proj_v[:, o, d, :], lax.Precision.HIGHEST)
    proj_high, proj_low = split(own_proj)
    proj_both = jnp.concatenate([own_proj, own_proj - proj_high.astype(F32)], axis=0).astype(BF16)

    def own(ref):
        lanes = lax.broadcasted_iota(jnp.int32, ref.shape, len(ref.shape) - 1)
        return [jnp.sum(jnp.where(lanes == 2 * row + c, ref[...], 0.0), axis=-1, keepdims=True) for c in range(2)]

    own_taps = own(taps_v)
    own_decay = own(decay_v)
    own_gain = own(gain_v)
    sub8 = lax.broadcasted_iota(jnp.int32, (8, 128), 0)
    decay_rows = jnp.zeros((8, 128), F32)
    start_rows = jnp.zeros((8, 128), F32)
    for o in range(2):
        for c in range(2):
            start_rows = jnp.where(sub8 == 4 * o + c, own_gain[c][o : o + 1], start_rows)
            for d in range(2):
                decay_rows = jnp.where(sub8 == 4 * o + 2 * d + c, own_decay[c][o, d : d + 1], decay_rows)
    lag8 = lax.broadcasted_iota(jnp.int32, (8, 128), 1)
    keep = ((sub8 >> 1) & 1) == 0

    def lags(step, carry):
        width = 1024
        block = table_v[:, pl.ds(pl.multiple_of(step * width, width), width)]
        parts = dot(layer, block)
        hidden = sine(parts[:64] + parts[64:128] + parts[128:])
        hid_high, hid_low = split(hidden)
        twice = dot(proj_both, hid_high)
        taps = twice[:8] + twice[8:] + dot(proj_high, hid_low)
        for i in range(width // 128):
            at = step * width + i * 128 + lag8
            piece = taps[:, 128 * i : 128 * (i + 1)] * jnp.exp(decay_rows * (at.astype(F32) * (-1.0 / (LENGTH - 1))))
            piece = jnp.where(at == 0, jnp.where(keep, piece + start_rows, 0.0), piece)
            to = ((i % 2) * 32 + i // 2 + step * 4) * 8
            lag_taps[pl.ds(pl.multiple_of(to, 8), 8), :] = piece
        return carry

    lax.fori_loop(0, LENGTH // 1024, lags, 0)

    twist = (twist_v[0], twist_v[1])
    inner_in = (inner_in_v[0], inner_in_v[1])
    inner_out = (inner_out_v[0], inner_out_v[1])
    for o in range(2):
        signals = jnp.concatenate([lag_taps[pl.ds(4 * o + k, 64, stride=8), :] for k in range(4)], axis=1)
        spectra[o] = filter_spectrum(signals, outer_in_v[...], twist, inner_in)
    tables = (outer_in_v[...], outer_out_v[...], twist, inner_in, inner_out)

    for part in range(2):
        blocks(part).wait_recv()
    first_hops, second_hops = hops(False), hops(True)
    for copy in first_hops:
        copy.start()
    for part in range(2):
        swap(part, 0).start()

    lane = lax.broadcasted_iota(jnp.int32, (128, 128), 1)
    sub = lax.broadcasted_iota(jnp.int32, (128, 128), 0)
    upper = (sub & 1) == 1
    after_me.wait_recv()
    before_me.wait_recv()
    double = jnp.where(lane == (sub >> 1), 1.0, 0.0)
    edge_before = dot_nt(double.astype(BF16), edge_in[0])[:, 1:2]
    edge_after = dot_nt(double.astype(BF16), edge_in[1])[:, 0:1]
    edge_before = jnp.where(row == 0, 0.0, edge_before)
    edge_after = jnp.where(row == ROWS - 1, 0.0, edge_after)
    role_taps = jnp.concatenate([taps_v[j, 2:3] for j in range(3)] + [jnp.zeros((5, 64), F32)], axis=0)
    columns = dot_nt(double[:, :64], role_taps, lax.Precision.HIGHEST)
    here = sort_v[:, 256:384]
    right, left = pltpu.roll(here, 1, 1), pltpu.roll(here, 127, 1)
    before = jnp.where(lane == 0, jnp.where(upper, pltpu.roll(right, 1, 0), edge_before), right)
    after = jnp.where(lane == 127, jnp.where(upper, edge_after, pltpu.roll(left, 127, 0)), left)
    second = before * columns[:, 0:1] + here * columns[:, 1:2] + after * columns[:, 2:3]
    gate = sort_v[:, 384:]
    gate_v[...] = second * (gate / (1.0 + jnp.exp(-gate)))

    lane = lax.broadcasted_iota(jnp.int32, (32, 128), 1)
    sub = lax.broadcasted_iota(jnp.int32, (32, 128), 0)

    def arrived(buffer):
        for r in range(ROWS):
            block_v[4 * r : 4 * r + 4, :] = buffer[r].astype(F32)

    def short(role):
        sides = []
        for c in range(2):
            here = [block_v[pl.ds(2 * c + h, 32, stride=4), :] for h in range(2)]
            before, after = shifted(here, lane, sub)
            weight = [own_taps[c][j, role : role + 1] for j in range(3)]
            sides.append(
                jnp.concatenate(
                    [before[h] * weight[0] + here[h] * weight[1] + after[h] * weight[2] for h in range(2)], axis=0
                )
            )
        return jnp.concatenate(sides, axis=1)

    whole(value_trip).wait_recv()
    arrived(recv1)
    conv = convolve(short(0), spectra[0], tables)
    whole(first_trip).wait_recv()
    arrived(recv2)
    conv = convolve(short(1) * conv, spectra[1], tables)

    for c in range(2):
        for h in range(2):
            back_v[pl.ds(2 * c + h, 32, stride=4), :] = conv[32 * h : 32 * (h + 1), 128 * c : 128 * (c + 1)]
    for r in range(ROWS):
        send3[r] = back_v[4 * r : 4 * r + 4, :].astype(BF16)
    recv3[pl.ds(row, 1)] = send3[pl.ds(row, 1)]
    row_peers(lambda r: to_row(back_trip, r).start())

    for copy in first_hops:
        copy.wait_recv()
    for copy in second_hops:
        copy.start()
    for part in range(2):
        for step in (1, 3):
            swap(part, step).start()

    i128 = lax.broadcasted_iota(jnp.int32, (128, 256), 0)
    l256 = lax.broadcasted_iota(jnp.int32, (128, 256), 1)
    spread = jnp.where(l256 == 128 * (i128 & 1) + 64 * lax.rem(col, 2) + (i128 >> 1), 1.0, 0.0).astype(BF16)
    whole(back_trip).wait_recv()
    arrived(recv3)
    flipped = jnp.transpose(block_v[...] * gate_v[...]).astype(BF16)
    rows = dot(flipped, spread).astype(BF16)
    for h in range(2):
        send4[8 * h : 8 * (h + 1)] = rows[:, 128 * h : 128 * (h + 1)].reshape(8, 16, 128)
    recv4[pl.ds(col, 1)] = send4[pl.ds(col, 1)]
    col_peers(lambda c: to_col(last_trip, c).start())

    for copy in second_hops:
        copy.wait_recv()
    for part in range(2):
        swap(part, 2).start()
    half = w_full.at[core]
    swapped = pltpu.make_async_remote_copy(
        src_ref=half, dst_ref=half, send_sem=swap_send, recv_sem=swap_recv,
        device_id=(partner, col), device_id_type=MESH,
    )
    swapped.wait_recv()
    whole(last_trip).wait_recv()
    left = jnp.concatenate([recv4[2 * m] + recv4[2 * m + 1] for m in range(8)], axis=1)
    for k in range(2):
        for part in range(2):
            at = 1024 * k + 512 * part
            out_ref[0, :, at : at + 512] = dot(left, w_full[k, part].reshape(1024, 512)).astype(BF16)

    for trip in (value_trip, first_trip, back_trip, last_trip):
        whole(trip).wait_send()
    after_me.wait_send()
    before_me.wait_send()
    for part in range(2):
        blocks(part).wait_send()
    for copy in first_hops + second_hops:
        copy.wait_send()
    swapped.wait_send()


def body(
    tokens, w_value, w_first, w_second, w_gate, conv_taps, filter_embed, filter_freq, filter_proj, filter_decay,
    skip_gain, w_out,
):
    consts = [jnp.asarray(c) for c in constants()]
    vmem = pltpu.VMEM
    sem = pltpu.SemaphoreType.DMA
    scratch = [
        vmem((256, 2048), BF16),
        vmem((256, 2048), BF16),
        vmem((3, 3, 64), F32),
        vmem((FEATS, 64), F32),
        vmem((1, 64), F32),
        vmem((64, 2, 2, 64), F32),
        vmem((2, 2, 64), F32),
        vmem((2, 64), F32),
        vmem((128, 192), BF16),
        vmem((64, 384), BF16),
        vmem((2, 64, 128), F32),
        vmem((2, 256, 256), BF16),
        vmem((2, 256, 256), BF16),
        vmem((128, LENGTH), BF16),
        vmem((2, 2, 4, 4, 64, 512), BF16),
        vmem((3, 128, 128), F32),
        vmem((512, 128), F32),
        vmem((2, 128, 256), F32),
        vmem((128, 512), F32),
        vmem((128, 128), F32),
        vmem((128, 128), F32),
        vmem((128, 128), F32),
        vmem((16, 128), BF16),
        vmem((2, 16, 128), BF16),
        vmem((ROWS, 4, 128), BF16), vmem((ROWS, 4, 128), BF16),
        vmem((ROWS, 4, 128), BF16), vmem((ROWS, 4, 128), BF16),
        vmem((ROWS, 4, 128), BF16), vmem((ROWS, 4, 128), BF16),
        vmem((COLS, 16, 128), BF16), vmem((COLS, 16, 128), BF16),
        sem((19,)),
        sem, sem, sem, sem, sem, sem, sem, sem,
        sem((2,)), sem((2,)), sem((2,)), sem((2,)), sem((2, 4)), sem((2, 4)), sem, sem,
    ]
    anywhere = pl.BlockSpec(memory_space=pltpu.HBM)
    return pl.pallas_call(
        kernel,
        out_shape=jax.ShapeDtypeStruct((1, 16, 2048), BF16),
        in_specs=[anywhere] * 18,
        out_specs=pl.BlockSpec(memory_space=pltpu.VMEM),
        scratch_shapes=scratch,
        compiler_params=pltpu.CompilerParams(
            collective_id=0, has_side_effects=True, vmem_limit_bytes=67043328
        ),
    )(
        tokens, w_value.T, w_first.T, w_second.T, w_gate.T, conv_taps, filter_embed, filter_freq.reshape(1, -1),
        filter_proj, filter_decay, skip_gain, w_out, *consts,
    )


def solution(mesh):
    placed = (
        P(None, "row", None),
        P(None, "col"),
        P(None, "col"),
        P(None, "col"),
        P(None, "col"),
        P(None, None, "col"),
        P(),
        P(),
        P(None, None, None, "col"),
        P(None, None, "col"),
        P(None, "col"),
        P("col", None),
    )
    return jax.shard_map(
        body, mesh=mesh, in_specs=placed, out_specs=P(None, ("row", "col"), None), check_vma=False
    )
```

```python
import functools
import math

import jax
import jax.numpy as jnp
import ml_dtypes
import numpy as np
from jax import lax
from jax.experimental import pallas as pl
from jax.experimental.pallas import tpu as pltpu
from jax.sharding import PartitionSpec as P

MESH = pl.DeviceIdType.MESH
F32 = jnp.float32
BF16 = jnp.bfloat16

LENGTH = 8192
ROWS = 32
COLS = 16
FEATS = 33
FEAT_STEP = 40


def halves(x):
    x = np.asarray(x, np.float64)
    high = x.astype(ml_dtypes.bfloat16)
    low = (x - high.astype(np.float64)).astype(ml_dtypes.bfloat16)
    return high, low


@functools.lru_cache(None)
def constants():
    two_pi = 2.0 * math.pi
    j = np.arange(64)
    q = 2 * (j % 32) + j // 32
    k1 = np.arange(64) + 0.5
    p = np.arange(128)
    first = np.concatenate([np.cos(two_pi * np.outer(k1, q) / 128), -np.sin(two_pi * np.outer(k1, q) / 128)], axis=0)
    f_high, f_low = halves(first)
    outer_in = np.concatenate([f_high, f_high, f_low], axis=1)
    outer_out = np.concatenate([f_high.T, f_high.T, f_low.T], axis=1)
    twist = np.stack(
        [np.cos(two_pi * np.outer(k1, p) / 16384), -np.sin(two_pi * np.outer(k1, p) / 16384)]
    ).astype(np.float32)
    g_real = np.cos(two_pi * (np.outer(p, p) % 128) / 128)
    g_imag = -np.sin(two_pi * (np.outer(p, p) % 128) / 128)
    inner_in = np.stack(halves(np.block([[g_real, g_imag], [-g_imag, g_real]])))
    inner_out = np.stack(halves(np.block([[g_real, -g_imag], [g_imag, g_real]])))
    n = np.arange(LENGTH)
    b = np.arange(1, 17)
    phase = two_pi * (np.outer(b, n) % LENGTH) / LENGTH
    features = np.concatenate([(n / (LENGTH - 1))[None], np.cos(phase), np.sin(phase)], axis=0)
    table = np.zeros((128, LENGTH), ml_dtypes.bfloat16)
    rest = features
    for part in range(3):
        piece = rest.astype(ml_dtypes.bfloat16)
        table[part * FEAT_STEP : part * FEAT_STEP + FEATS] = piece
        rest = rest - piece.astype(np.float64)
    return outer_in, outer_out, twist, inner_in, inner_out, table


def split(x):
    high = x.astype(BF16)
    return high, (x - high.astype(F32)).astype(BF16)


def dot(a, b):
    return jnp.dot(a, b, preferred_element_type=F32)


def dot_nt(a, b, precision=None):
    return lax.dot_general(a, b, (((1,), (1,)), ((), ())), precision=precision, preferred_element_type=F32)


def times(x, matrix):
    high, low = split(x)
    return dot(high, matrix[0]) + dot(low, matrix[0]) + dot(high, matrix[1])


def forward(signal, outer_in, twist, inner_in):
    high, low = split(signal)
    stage = dot(outer_in, jnp.concatenate([high, low, high], axis=0))
    turned = []
    for m in range(signal.shape[1] // 128):
        real = stage[:64, 128 * m : 128 * (m + 1)]
        imag = stage[64:, 128 * m : 128 * (m + 1)]
        turned.append(
            jnp.concatenate([real * twist[0] - imag * twist[1], real * twist[1] + imag * twist[0]], axis=1)
        )
    return times(jnp.concatenate(turned, axis=0), inner_in)


def inverse(spectrum, outer_out, twist, inner_out):
    stage = times(spectrum, inner_out)
    reals, imags = [], []
    for m in range(spectrum.shape[0] // 64):
        real = stage[64 * m : 64 * (m + 1), :128]
        imag = stage[64 * m : 64 * (m + 1), 128:]
        reals.append(real * twist[0] + imag * twist[1])
        imags.append(imag * twist[0] - real * twist[1])
    both = jnp.concatenate([jnp.concatenate(reals, axis=1), jnp.concatenate(imags, axis=1)], axis=0)
    high, low = split(both)
    return dot(outer_out, jnp.concatenate([high, low, high], axis=0))


def convolve(signal, filt, tables):
    outer_in, outer_out, twist, inner_in, inner_out = tables
    spectrum = forward(signal, outer_in, twist, inner_in)
    real, imag = spectrum[:, :128], spectrum[:, 128:]
    f_real, f_imag = filt[:, :128], filt[:, 128:]
    product = jnp.concatenate([real * f_real - imag * f_imag, real * f_imag + imag * f_real], axis=1)
    return inverse(product, outer_out, twist, inner_out)


def filter_spectrum(signals, outer_in, twist, inner_in):
    spectra = forward(signals, outer_in, twist, inner_in)
    ahead, behind = spectra[:128], spectra[128:]
    scale = 2.0 / (2 * LENGTH)
    return jnp.concatenate(
        [(ahead[:, :128] + behind[:, :128]) * scale, (ahead[:, 128:] - behind[:, 128:]) * scale], axis=1
    )


def sine(x):
    k = jnp.floor(x * (1.0 / math.pi) + 0.5)
    r = x - k * 3.140625
    r = r - k * 9.67502593994140625e-4
    r = r - k * 1.509957990978376432e-7
    half = k * 0.5
    sign = 1.0 - 4.0 * (half - jnp.floor(half))
    s = r * r
    poly = -1.0 / 39916800.0
    for c in (1.0 / 362880.0, -1.0 / 5040.0, 1.0 / 120.0, -1.0 / 6.0):
        poly = poly * s + c
    return sign * (r + r * (s * poly))


def shifted(parts, lane, sub):
    right = [pltpu.roll(x, 1, 1) for x in parts]
    left = [pltpu.roll(x, 127, 1) for x in parts]
    carry = jnp.where(sub == 0, 0.0, pltpu.roll(right[1], 1, 0))
    back = jnp.where(sub == 31, 0.0, pltpu.roll(left[0], 31, 0))
    before = [jnp.where(lane == 0, carry, right[0]), jnp.where(lane == 0, right[0], right[1])]
    after = [jnp.where(lane == 127, left[1], left[0]), jnp.where(lane == 127, back, left[1])]
    return before, after


def kernel(
    tokens, w_value, w_first, w_second, w_gate, conv_taps, embed, freq, proj, decay, gain, w_out,
    outer_in_h, outer_out_h, twist_h, inner_in_h, inner_out_h, table_h,
    out_ref,
    tok_v, w_v, taps_v, embed_v, freq_v, proj_v, decay_v, gain_v,
    outer_in_v, outer_out_v, twist_v, inner_in_v, inner_out_v, table_v,
    w_full, est, lag_taps, spectra, sort_v, gate_v, block_v, back_v, edge_out, edge_in,
    send1, recv1, send2, recv2, send3, recv3, send4, recv4, total,
    load_sem, send_sem1, recv_sem1, send_sem2, recv_sem2, send_sem3, recv_sem3, send_sem4, recv_sem4,
    edge_send, edge_recv, block_send, block_recv, hop_send, hop_recv, pass_send, pass_recv, swap_send, swap_recv,
):
    row = lax.axis_index("row")
    col = lax.axis_index("col")
    z = lax.div(row, 2)
    core = lax.rem(row, 2)
    partner = z * 2 + 1 - core
    y = lax.div(col, 4)
    x = lax.rem(col, 4)

    def row_peers(visit):
        def step(i, carry):
            away = 8 + lax.div(i + 1, 2) * (1 - 2 * lax.rem(i, 2))
            there = lax.rem(z + away, 16) * 2
            visit(there)
            visit(there + 1)
            return carry

        lax.fori_loop(0, 15, step, 0)
        visit(partner)

    def col_peers(visit):
        def step(i, carry):
            visit(lax.rem(col + i, COLS))
            return carry

        lax.fori_loop(1, COLS, step, 0)

    barrier = pltpu.get_barrier_semaphore()
    row_peers(lambda r: pl.semaphore_signal(barrier, inc=1, device_id=(r, col), device_id_type=MESH))
    col_peers(lambda c: pl.semaphore_signal(barrier, inc=1, device_id=(row, c), device_id_type=MESH))

    loads = []
    for source, target in (
        (tokens.at[0], tok_v),
        (w_value, w_v.at[pl.ds(0, 64)]),
        (w_first, w_v.at[pl.ds(64, 64)]),
        (w_second, w_v.at[pl.ds(128, 64)]),
        (w_gate, w_v.at[pl.ds(192, 64)]),
        (w_out.at[:, pl.ds(pl.multiple_of(core * 1024, 512), 512)], w_full.at[core, 0, y, x]),
        (w_out.at[:, pl.ds(pl.multiple_of(core * 1024 + 512, 512), 512)], w_full.at[core, 1, y, x]),
        (conv_taps, taps_v),
        (embed, embed_v),
        (freq, freq_v),
        (proj, proj_v),
        (decay, decay_v),
        (gain, gain_v),
        (table_h, table_v),
        (outer_in_h, outer_in_v),
        (outer_out_h, outer_out_v),
        (twist_h, twist_v),
        (inner_in_h, inner_in_v),
        (inner_out_h, inner_out_v),
    ):
        load = pltpu.make_async_copy(source, target, load_sem.at[len(loads)])
        load.start()
        loads.append(load)

    for load in loads[:5]:
        load.wait()
    result = dot_nt(w_v[...], tok_v[...]).astype(BF16)
    order = lax.broadcasted_iota(jnp.int32, (128, 128), 0)
    source = lax.broadcasted_iota(jnp.int32, (128, 128), 1)
    place = jnp.where(source == (order & 1) * 64 + (order >> 1), 1.0, 0.0).astype(BF16)
    roles = [
        jnp.concatenate([result[64 * k : 64 * (k + 1), :128], result[64 * k : 64 * (k + 1), 128:]], axis=0)
        for k in range(4)
    ]
    sort_v[...] = dot(place, jnp.concatenate(roles, axis=1))
    for r in range(ROWS):
        send1[r] = sort_v[4 * r : 4 * r + 4, :128].astype(BF16)
        send2[r] = sort_v[4 * r : 4 * r + 4, 128:256].astype(BF16)
    recv1[pl.ds(row, 1)] = send1[pl.ds(row, 1)]
    recv2[pl.ds(row, 1)] = send2[pl.ds(row, 1)]
    end_row = lax.broadcasted_iota(jnp.int32, (16, 256), 0)
    end_col = lax.broadcasted_iota(jnp.int32, (16, 256), 1)
    ends = jnp.where(end_col == 255 * end_row, 1.0, 0.0).astype(BF16)
    edge_out[...] = dot_nt(ends, result[128:]).astype(BF16)
    loads[5].wait()
    loads[6].wait()

    def to_row(trip, r):
        source, target, sent, received = trip
        return pltpu.make_async_remote_copy(
            src_ref=source.at[r], dst_ref=target.at[row], send_sem=sent, recv_sem=received,
            device_id=(r, col), device_id_type=MESH,
        )

    def whole(trip):
        source, target, sent, received = trip
        count = pl.ds(0, source.shape[0] - 1)
        return pltpu.make_async_remote_copy(
            src_ref=source.at[count], dst_ref=target.at[count], send_sem=sent, recv_sem=received,
            device_id=(partner, col), device_id_type=MESH,
        )

    def edge(step, slot):
        return pltpu.make_async_remote_copy(
            src_ref=edge_out, dst_ref=edge_in.at[slot], send_sem=edge_send.at[slot], recv_sem=edge_recv.at[slot],
            device_id=(lax.rem(row + step, ROWS), col), device_id_type=MESH,
        )

    after_me, before_me = edge(1, 0), edge(ROWS - 1, 1)

    def block(part, step):
        if part == 0:
            return w_full.at[core, 0, y, lax.rem(x + step, 4)]
        return w_full.at[core, 1, lax.rem(y + step, 4), x]

    def group(part, step, half=None):
        some = slice(None) if half is None else pl.ds(2 * half, 2)
        if part == 0:
            return w_full.at[core, 0, lax.rem(y + step, 4), some]
        return w_full.at[core, 1, some, lax.rem(x + step, 4)]

    def along(part, step):
        return y * 4 + lax.rem(x + step, 4) if part == 0 else lax.rem(y + step, 4) * 4 + x

    def spread_block(part, step):
        here = block(part, 0)
        return pltpu.make_async_remote_copy(
            src_ref=here, dst_ref=here, send_sem=block_send.at[part, step],
            recv_sem=block_recv.at[part, step], device_id=(row, along(part, step)), device_id_type=MESH,
        )

    def hop_block(part, side, step):
        here = block(part, step)
        return pltpu.make_async_remote_copy(
            src_ref=here, dst_ref=here, send_sem=hop_send.at[part, side], recv_sem=hop_recv.at[part, side],
            device_id=(row, along(1 - part, 1 + 2 * side)), device_id_type=MESH,
        )

    def hopped(part, side):
        here = group(part, 3 - 2 * side)
        return pltpu.make_async_remote_copy(
            src_ref=here, dst_ref=here, send_sem=hop_send.at[part, side], recv_sem=hop_recv.at[part, side],
            device_id=(row, along(1 - part, 1 + 2 * side)), device_id_type=MESH,
        )

    def pass_on(part, side):
        here = group(part, 3 - 2 * side, side)
        return pltpu.make_async_remote_copy(
            src_ref=here, dst_ref=here, send_sem=pass_send.at[part, side], recv_sem=pass_recv.at[part, side],
            device_id=(row, along(1 - part, 1 + 2 * side)), device_id_type=MESH,
        )

    both = [(part, side) for part in range(2) for side in range(2)]

    def swap(part, step):
        here = group(part, step)
        return pltpu.make_async_remote_copy(
            src_ref=here, dst_ref=here, send_sem=swap_send, recv_sem=swap_recv,
            device_id=(partner, col), device_id_type=MESH,
        )

    value_trip = (send1, recv1, send_sem1, recv_sem1)
    first_trip = (send2, recv2, send_sem2, recv_sem2)
    back_trip = (send3, recv3, send_sem3, recv_sem3)
    last_trip = (send4, recv4, send_sem4, recv_sem4.at[0])

    pl.semaphore_wait(barrier, ROWS - 1 + COLS - 1)
    row_peers(lambda r: to_row(value_trip, r).start())
    for step in (1, 3, 2):
        for part in range(2):
            spread_block(part, step).start()
    for part, side in both:
        hop_block(part, side, 0).start()
    row_peers(lambda r: to_row(first_trip, r).start())
    after_me.start()
    before_me.start()

    for load in loads[7:]:
        load.wait()
    scaled = embed_v[...] * freq_v[...]
    est[...] = jnp.zeros_like(est)
    high = scaled.astype(BF16).astype(F32)
    rest = scaled - high
    mid = rest.astype(BF16).astype(F32)
    low = rest - mid
    for k, parts in enumerate(((high, high, high), (mid, mid), (low,))):
        for m, part in enumerate(parts):
            est[k, FEAT_STEP * m : FEAT_STEP * m + FEATS, :64] = part
    layer = jnp.concatenate([jnp.transpose(est[k])[:64] for k in range(3)], axis=0).astype(BF16)

    lane64 = lax.broadcasted_iota(jnp.int32, (8, 64), 1)
    sub64 = lax.broadcasted_iota(jnp.int32, (8, 64), 0)
    own_proj = jnp.zeros((8, 64), F32)
    for o in range(2):
        for d in range(2):
            pick = jnp.where((lane64 == 2 * row + (sub64 & 1)) & ((sub64 >> 1) == 2 * o + d), 1.0, 0.0)
            own_proj = own_proj + dot_nt(pick, proj_v[:, o, d, :], lax.Precision.HIGHEST)
    proj_high, proj_low = split(own_proj)
    proj_both = jnp.concatenate([own_proj, own_proj - proj_high.astype(F32)], axis=0).astype(BF16)

    def own(ref):
        lanes = lax.broadcasted_iota(jnp.int32, ref.shape, len(ref.shape) - 1)
        return [jnp.sum(jnp.where(lanes == 2 * row + c, ref[...], 0.0), axis=-1, keepdims=True) for c in range(2)]

    own_taps = own(taps_v)
    own_decay = own(decay_v)
    own_gain = own(gain_v)
    sub8 = lax.broadcasted_iota(jnp.int32, (8, 128), 0)
    decay_rows = jnp.zeros((8, 128), F32)
    start_rows = jnp.zeros((8, 128), F32)
    for o in range(2):
        for c in range(2):
            start_rows = jnp.where(sub8 == 4 * o + c, own_gain[c][o : o + 1], start_rows)
            for d in range(2):
                decay_rows = jnp.where(sub8 == 4 * o + 2 * d + c, own_decay[c][o, d : d + 1], decay_rows)
    lag8 = lax.broadcasted_iota(jnp.int32, (8, 128), 1)
    keep = ((sub8 >> 1) & 1) == 0

    def lags(step, carry):
        width = 1024
        block = table_v[:, pl.ds(pl.multiple_of(step * width, width), width)]
        parts = dot(layer, block)
        hidden = sine(parts[:64] + parts[64:128] + parts[128:])
        hid_high, hid_low = split(hidden)
        twice = dot(proj_both, hid_high)
        taps = twice[:8] + twice[8:] + dot(proj_high, hid_low)
        for i in range(width // 128):
            at = step * width + i * 128 + lag8
            piece = taps[:, 128 * i : 128 * (i + 1)] * jnp.exp(decay_rows * (at.astype(F32) * (-1.0 / (LENGTH - 1))))
            piece = jnp.where(at == 0, jnp.where(keep, piece + start_rows, 0.0), piece)
            to = ((i % 2) * 32 + i // 2 + step * 4) * 8
            lag_taps[pl.ds(pl.multiple_of(to, 8), 8), :] = piece
        return carry

    lax.fori_loop(0, LENGTH // 1024, lags, 0)

    twist = (twist_v[0], twist_v[1])
    inner_in = (inner_in_v[0], inner_in_v[1])
    inner_out = (inner_out_v[0], inner_out_v[1])
    for o in range(2):
        signals = jnp.concatenate([lag_taps[pl.ds(4 * o + k, 64, stride=8), :] for k in range(4)], axis=1)
        spectra[o] = filter_spectrum(signals, outer_in_v[...], twist, inner_in)
    tables = (outer_in_v[...], outer_out_v[...], twist, inner_in, inner_out)

    for step in (1, 3, 2):
        for part in range(2):
            spread_block(part, step).wait_recv()
        for part, side in both:
            hop_block(part, side, 4 - step).start()
    for part in range(2):
        swap(part, 0).start()

    lane = lax.broadcasted_iota(jnp.int32, (32, 128), 1)
    sub = lax.broadcasted_iota(jnp.int32, (32, 128), 0)

    def arrived(buffer):
        for r in range(ROWS):
            block_v[4 * r : 4 * r + 4, :] = buffer[r].astype(F32)

    def short(role):
        sides = []
        for c in range(2):
            here = [block_v[pl.ds(2 * c + h, 32, stride=4), :] for h in range(2)]
            before, after = shifted(here, lane, sub)
            weight = [own_taps[c][j, role : role + 1] for j in range(3)]
            sides.append(
                jnp.concatenate(
                    [before[h] * weight[0] + here[h] * weight[1] + after[h] * weight[2] for h in range(2)], axis=0
                )
            )
        return jnp.concatenate(sides, axis=1)

    whole(value_trip).wait_recv()
    arrived(recv1)
    conv = convolve(short(0), spectra[0], tables)
    whole(first_trip).wait_recv()
    arrived(recv2)
    conv = convolve(short(1) * conv, spectra[1], tables)

    for c in range(2):
        for h in range(2):
            back_v[pl.ds(2 * c + h, 32, stride=4), :] = conv[32 * h : 32 * (h + 1), 128 * c : 128 * (c + 1)]
    for r in range(ROWS):
        send3[r] = back_v[4 * r : 4 * r + 4, :].astype(BF16)
    recv3[pl.ds(row, 1)] = send3[pl.ds(row, 1)]
    row_peers(lambda r: to_row(back_trip, r).start())

    lane = lax.broadcasted_iota(jnp.int32, (128, 128), 1)
    sub = lax.broadcasted_iota(jnp.int32, (128, 128), 0)
    upper = (sub & 1) == 1
    after_me.wait_recv()
    before_me.wait_recv()
    double = jnp.where(lane == (sub >> 1), 1.0, 0.0)
    edge_before = dot_nt(double.astype(BF16), edge_in[0])[:, 1:2]
    edge_after = dot_nt(double.astype(BF16), edge_in[1])[:, 0:1]
    edge_before = jnp.where(row == 0, 0.0, edge_before)
    edge_after = jnp.where(row == ROWS - 1, 0.0, edge_after)
    role_taps = jnp.concatenate([taps_v[j, 2:3] for j in range(3)] + [jnp.zeros((5, 64), F32)], axis=0)
    columns = dot_nt(double[:, :64], role_taps, lax.Precision.HIGHEST)
    here = sort_v[:, 256:384]
    right, left = pltpu.roll(here, 1, 1), pltpu.roll(here, 127, 1)
    before = jnp.where(lane == 0, jnp.where(upper, pltpu.roll(right, 1, 0), edge_before), right)
    after = jnp.where(lane == 127, jnp.where(upper, edge_after, pltpu.roll(left, 127, 0)), left)
    second = before * columns[:, 0:1] + here * columns[:, 1:2] + after * columns[:, 2:3]
    gate = sort_v[:, 384:]
    gate_v[...] = second * (gate / (1.0 + jnp.exp(-gate)))

    for part, side in both:
        hopped(part, side).wait_recv()
    for part, side in both:
        pass_on(part, side).start()
    for part in range(2):
        for step in (1, 3):
            swap(part, step).start()

    p128 = lax.broadcasted_iota(jnp.int32, (128, 256), 0)
    l256 = lax.broadcasted_iota(jnp.int32, (128, 256), 1)
    spread = jnp.where((l256 >> 7 == (p128 & 1)) & ((l256 & 63) == (p128 >> 1)), 1.0, 0.0).astype(BF16)
    whole(back_trip).wait_recv()
    arrived(recv3)
    flipped = jnp.transpose(block_v[...] * gate_v[...]).astype(BF16)
    rows = dot(flipped, spread)
    low_first = (lax.broadcasted_iota(jnp.int32, (8, 8, 128), 2) < 64) == (lax.rem(col, 2) == 0)
    for h in range(2):
        tiles = rows[:, 128 * h : 128 * (h + 1)].reshape(8, 2, 8, 128)
        send4[8 * h : 8 * (h + 1)] = jnp.where(low_first, tiles[:, 0], tiles[:, 1]).astype(BF16)
    recv4[pl.ds(col, 1)] = send4[pl.ds(col, 1)]

    def last(step_y, step_x):
        c = lax.rem(y + step_y, 4) * 4 + lax.rem(x + step_x, 4)
        return pltpu.make_async_remote_copy(
            src_ref=send4.at[c], dst_ref=recv4.at[col], send_sem=send_sem4, recv_sem=recv_sem4.at[(4 - step_y) % 4],
            device_id=(row, c), device_id_type=MESH,
        )

    def last_group(step_y):
        some = recv4.at[pl.ds(0, 4 if step_y else 3)]
        return pltpu.make_async_remote_copy(
            src_ref=some, dst_ref=some, send_sem=send_sem4, recv_sem=recv_sem4.at[step_y],
            device_id=(partner, col), device_id_type=MESH,
        )

    for step_y in (2, 1, 3, 0):
        for step_x in (2, 1, 3, 0):
            if step_y or step_x:
                last(step_y, step_x).start()

    for part, side in both:
        pass_on(part, side).wait_recv()
    for part in range(2):
        swap(part, 2).start()
    half = w_full.at[core]
    swapped = pltpu.make_async_remote_copy(
        src_ref=half, dst_ref=half, send_sem=swap_send, recv_sem=swap_recv,
        device_id=(partner, col), device_id_type=MESH,
    )
    swapped.wait_recv()
    low_lanes = lax.broadcasted_iota(jnp.int32, (8, 128), 1) < 64
    for step_y in (0, 1, 3, 2):
        last_group(step_y).wait_recv()
        yy = lax.rem(y + step_y, 4)
        lefts = []
        for m in range(2):
            even, odd = (recv4[4 * yy + 2 * m + e].astype(F32) for e in range(2))
            upper_rows = jnp.where(low_lanes, even, odd)
            lower_rows = pltpu.roll(jnp.where(low_lanes, odd, even), 64, 1)
            lefts.append(jnp.concatenate([upper_rows, lower_rows], axis=0))
        left = jnp.concatenate(lefts, axis=1).astype(BF16)
        for k in range(2):
            for part in range(2):
                at = 1024 * k + 512 * part
                term = dot(left, w_full[k, part, yy].reshape(256, 512))
                if step_y:
                    term = term + total[:, at : at + 512]
                if step_y == 2:
                    out_ref[0, :, at : at + 512] = term.astype(BF16)
                else:
                    total[:, at : at + 512] = term

    for trip in (value_trip, first_trip, back_trip, last_trip):
        whole(trip).wait_send()
    after_me.wait_send()
    before_me.wait_send()
    for part in range(2):
        for step in (1, 2, 3):
            spread_block(part, step).wait_send()
    for part, side in both:
        hopped(part, side).wait_send()
        pass_on(part, side).wait_send()
    swapped.wait_send()


def body(
    tokens, w_value, w_first, w_second, w_gate, conv_taps, filter_embed, filter_freq, filter_proj, filter_decay,
    skip_gain, w_out,
):
    consts = [jnp.asarray(c) for c in constants()]
    vmem = pltpu.VMEM
    sem = pltpu.SemaphoreType.DMA
    scratch = [
        vmem((256, 2048), BF16),
        vmem((256, 2048), BF16),
        vmem((3, 3, 64), F32),
        vmem((FEATS, 64), F32),
        vmem((1, 64), F32),
        vmem((64, 2, 2, 64), F32),
        vmem((2, 2, 64), F32),
        vmem((2, 64), F32),
        vmem((128, 192), BF16),
        vmem((64, 384), BF16),
        vmem((2, 64, 128), F32),
        vmem((2, 256, 256), BF16),
        vmem((2, 256, 256), BF16),
        vmem((128, LENGTH), BF16),
        vmem((2, 2, 4, 4, 64, 512), BF16),
        vmem((3, 128, 128), F32),
        vmem((512, 128), F32),
        vmem((2, 128, 256), F32),
        vmem((128, 512), F32),
        vmem((128, 128), F32),
        vmem((128, 128), F32),
        vmem((128, 128), F32),
        vmem((16, 128), BF16),
        vmem((2, 16, 128), BF16),
        vmem((ROWS, 4, 128), BF16), vmem((ROWS, 4, 128), BF16),
        vmem((ROWS, 4, 128), BF16), vmem((ROWS, 4, 128), BF16),
        vmem((ROWS, 4, 128), BF16), vmem((ROWS, 4, 128), BF16),
        vmem((COLS, 8, 128), BF16), vmem((COLS, 8, 128), BF16),
        vmem((16, 2048), F32),
        sem((19,)),
        sem, sem, sem, sem, sem, sem, sem, sem((4,)),
        sem((2,)), sem((2,)), sem((2, 4)), sem((2, 4)), sem((2, 2)), sem((2, 2)), sem((2, 2)), sem((2, 2)), sem, sem,
    ]
    anywhere = pl.BlockSpec(memory_space=pltpu.HBM)
    return pl.pallas_call(
        kernel,
        out_shape=jax.ShapeDtypeStruct((1, 16, 2048), BF16),
        in_specs=[anywhere] * 18,
        out_specs=pl.BlockSpec(memory_space=pltpu.VMEM),
        scratch_shapes=scratch,
        compiler_params=pltpu.CompilerParams(
            collective_id=0, has_side_effects=True, vmem_limit_bytes=48 * 1024 * 1024
        ),
    )(*[
        pltpu.with_memory_space_constraint(operand, pltpu.HBM)
        for operand in (
            tokens, w_value.T, w_first.T, w_second.T, w_gate.T, conv_taps, filter_embed, filter_freq.reshape(1, -1),
            filter_proj, filter_decay, skip_gain, w_out, *consts,
        )
    ])


def solution(mesh):
    placed = (
        P(None, "row", None),
        P(None, "col"),
        P(None, "col"),
        P(None, "col"),
        P(None, "col"),
        P(None, None, "col"),
        P(),
        P(),
        P(None, None, None, "col"),
        P(None, None, "col"),
        P(None, "col"),
        P("col", None),
    )
    return jax.shard_map(
        body, mesh=mesh, in_specs=placed, out_specs=P(None, ("row", "col"), None), check_vma=False
    )
```

```python
import functools
import math

import jax
import jax.numpy as jnp
import ml_dtypes
import numpy as np
from jax import lax
from jax.experimental import pallas as pl
from jax.experimental.pallas import tpu as pltpu
from jax.sharding import PartitionSpec as P

MESH = pl.DeviceIdType.MESH
F32 = jnp.float32
BF16 = jnp.bfloat16

LENGTH = 8192
ROWS = 32
COLS = 16
FEATS = 33
FEAT_STEP = 40


def halves(x):
    x = np.asarray(x, np.float64)
    high = x.astype(ml_dtypes.bfloat16)
    low = (x - high.astype(np.float64)).astype(ml_dtypes.bfloat16)
    return high, low


@functools.lru_cache(None)
def constants():
    two_pi = 2.0 * math.pi
    j = np.arange(64)
    q = 2 * (j % 32) + j // 32
    k1 = np.arange(64) + 0.5
    p = np.arange(128)
    first = np.concatenate([np.cos(two_pi * np.outer(k1, q) / 128), -np.sin(two_pi * np.outer(k1, q) / 128)], axis=0)
    f_high, f_low = halves(first)
    outer_in = np.concatenate([f_high, f_high, f_low], axis=1)
    outer_out = np.concatenate([f_high.T, f_high.T, f_low.T], axis=1)
    twist = np.stack(
        [np.cos(two_pi * np.outer(k1, p) / 16384), -np.sin(two_pi * np.outer(k1, p) / 16384)]
    ).astype(np.float32)
    g_real = np.cos(two_pi * (np.outer(p, p) % 128) / 128)
    g_imag = -np.sin(two_pi * (np.outer(p, p) % 128) / 128)
    inner_in = np.stack(halves(np.block([[g_real, g_imag], [-g_imag, g_real]])))
    inner_out = np.stack(halves(np.block([[g_real, -g_imag], [g_imag, g_real]])))
    n = np.arange(LENGTH)
    b = np.arange(1, 17)
    phase = two_pi * (np.outer(b, n) % LENGTH) / LENGTH
    features = np.concatenate([(n / (LENGTH - 1))[None], np.cos(phase), np.sin(phase)], axis=0)
    table = np.zeros((128, LENGTH), ml_dtypes.bfloat16)
    rest = features
    for part in range(3):
        piece = rest.astype(ml_dtypes.bfloat16)
        table[part * FEAT_STEP : part * FEAT_STEP + FEATS] = piece
        rest = rest - piece.astype(np.float64)
    return outer_in, outer_out, twist, inner_in, inner_out, table


def split(x):
    high = x.astype(BF16)
    return high, (x - high.astype(F32)).astype(BF16)


def dot(a, b):
    return jnp.dot(a, b, preferred_element_type=F32)


def dot_nt(a, b, precision=None):
    return lax.dot_general(a, b, (((1,), (1,)), ((), ())), precision=precision, preferred_element_type=F32)


def times(x, matrix):
    high, low = split(x)
    return dot(high, matrix[0]) + dot(low, matrix[0]) + dot(high, matrix[1])


def forward(signal, outer_in, twist, inner_in):
    high, low = split(signal)
    stage = dot(outer_in, jnp.concatenate([high, low, high], axis=0))
    turned = []
    for m in range(signal.shape[1] // 128):
        real = stage[:64, 128 * m : 128 * (m + 1)]
        imag = stage[64:, 128 * m : 128 * (m + 1)]
        turned.append(
            jnp.concatenate([real * twist[0] - imag * twist[1], real * twist[1] + imag * twist[0]], axis=1)
        )
    return times(jnp.concatenate(turned, axis=0), inner_in)


def inverse(spectrum, outer_out, twist, inner_out):
    stage = times(spectrum, inner_out)
    reals, imags = [], []
    for m in range(spectrum.shape[0] // 64):
        real = stage[64 * m : 64 * (m + 1), :128]
        imag = stage[64 * m : 64 * (m + 1), 128:]
        reals.append(real * twist[0] + imag * twist[1])
        imags.append(imag * twist[0] - real * twist[1])
    both = jnp.concatenate([jnp.concatenate(reals, axis=1), jnp.concatenate(imags, axis=1)], axis=0)
    high, low = split(both)
    return dot(outer_out, jnp.concatenate([high, low, high], axis=0))


def convolve(signal, filt, tables):
    outer_in, outer_out, twist, inner_in, inner_out = tables
    spectrum = forward(signal, outer_in, twist, inner_in)
    real, imag = spectrum[:, :128], spectrum[:, 128:]
    f_real, f_imag = filt[:, :128], filt[:, 128:]
    product = jnp.concatenate([real * f_real - imag * f_imag, real * f_imag + imag * f_real], axis=1)
    return inverse(product, outer_out, twist, inner_out)


def filter_spectrum(signals, outer_in, twist, inner_in):
    spectra = forward(signals, outer_in, twist, inner_in)
    ahead, behind = spectra[:128], spectra[128:]
    scale = 2.0 / (2 * LENGTH)
    return jnp.concatenate(
        [(ahead[:, :128] + behind[:, :128]) * scale, (ahead[:, 128:] - behind[:, 128:]) * scale], axis=1
    )


def sine(x):
    k = jnp.floor(x * (1.0 / math.pi) + 0.5)
    r = x - k * 3.140625
    r = r - k * 9.67502593994140625e-4
    r = r - k * 1.509957990978376432e-7
    half = k * 0.5
    sign = 1.0 - 4.0 * (half - jnp.floor(half))
    s = r * r
    poly = -1.0 / 39916800.0
    for c in (1.0 / 362880.0, -1.0 / 5040.0, 1.0 / 120.0, -1.0 / 6.0):
        poly = poly * s + c
    return sign * (r + r * (s * poly))


def shifted(parts, lane, sub):
    right = [pltpu.roll(x, 1, 1) for x in parts]
    left = [pltpu.roll(x, 127, 1) for x in parts]
    carry = jnp.where(sub == 0, 0.0, pltpu.roll(right[1], 1, 0))
    back = jnp.where(sub == 31, 0.0, pltpu.roll(left[0], 31, 0))
    before = [jnp.where(lane == 0, carry, right[0]), jnp.where(lane == 0, right[0], right[1])]
    after = [jnp.where(lane == 127, left[1], left[0]), jnp.where(lane == 127, back, left[1])]
    return before, after


def kernel(
    tokens, w_value, w_first, w_second, w_gate, conv_taps, embed, freq, proj, decay, gain, w_out,
    outer_in_h, outer_out_h, twist_h, inner_in_h, inner_out_h, table_h,
    out_ref,
    tok_v, w_v, taps_v, embed_v, freq_v, proj_v, decay_v, gain_v,
    outer_in_v, outer_out_v, twist_v, inner_in_v, inner_out_v, table_v,
    w_full, est, lag_taps, spectra, sort_v, gate_v, block_v, back_v, edge_out, edge_in,
    send1, recv1, send2, recv2, send3, recv3, send4, recv4, total, relay1, relay2,
    load_sem, send_sem1, recv_sem1, send_sem2, recv_sem2, send_sem3, recv_sem3, send_sem4, recv_sem4,
    edge_send, edge_recv, block_send, block_recv, hop_send, hop_recv, pass_send, pass_recv, swap_send, swap_recv,
    relay_send, relay_recv,
):
    row = lax.axis_index("row")
    col = lax.axis_index("col")
    z = lax.div(row, 2)
    core = lax.rem(row, 2)
    partner = z * 2 + 1 - core
    y = lax.div(col, 4)
    x = lax.rem(col, 4)

    def row_peers(visit):
        def step(i, carry):
            away = 8 + lax.div(i + 1, 2) * (1 - 2 * lax.rem(i, 2))
            there = lax.rem(z + away, 16) * 2
            visit(there)
            visit(there + 1)
            return carry

        lax.fori_loop(0, 15, step, 0)
        visit(partner)

    def near_peers(visit):
        def step(i, carry):
            away = 4 - lax.div(i, 2)
            there = lax.rem(z + 16 + away * (1 - 2 * lax.rem(i, 2)), 16) * 2
            visit(there)
            visit(there + 1)
            return carry

        lax.fori_loop(0, 8, step, 0)
        visit(partner)

    def col_peers(visit):
        def step(i, carry):
            visit(lax.rem(col + i, COLS))
            return carry

        lax.fori_loop(1, COLS, step, 0)

    barrier = pltpu.get_barrier_semaphore()
    near_peers(lambda r: pl.semaphore_signal(barrier, inc=1, device_id=(r, col), device_id_type=MESH))
    col_peers(lambda c: pl.semaphore_signal(barrier, inc=1, device_id=(row, c), device_id_type=MESH))

    loads = []
    for source, target in (
        (tokens.at[0], tok_v),
        (w_value, w_v.at[pl.ds(0, 64)]),
        (w_first, w_v.at[pl.ds(64, 64)]),
        (w_second, w_v.at[pl.ds(128, 64)]),
        (w_gate, w_v.at[pl.ds(192, 64)]),
        (w_out.at[:, pl.ds(pl.multiple_of(core * 1024, 512), 512)], w_full.at[core, 0, y, x]),
        (w_out.at[:, pl.ds(pl.multiple_of(core * 1024 + 512, 512), 512)], w_full.at[core, 1, y, x]),
        (conv_taps, taps_v),
        (embed, embed_v),
        (freq, freq_v),
        (proj, proj_v),
        (decay, decay_v),
        (gain, gain_v),
        (table_h, table_v),
        (outer_in_h, outer_in_v),
        (outer_out_h, outer_out_v),
        (twist_h, twist_v),
        (inner_in_h, inner_in_v),
        (inner_out_h, inner_out_v),
    ):
        load = pltpu.make_async_copy(source, target, load_sem.at[len(loads)])
        load.start()
        loads.append(load)

    for load in loads[:5]:
        load.wait()
    result = dot_nt(w_v[...], tok_v[...]).astype(BF16)
    order = lax.broadcasted_iota(jnp.int32, (128, 128), 0)
    source = lax.broadcasted_iota(jnp.int32, (128, 128), 1)
    place = jnp.where(source == (order & 1) * 64 + (order >> 1), 1.0, 0.0).astype(BF16)
    roles = [
        jnp.concatenate([result[64 * k : 64 * (k + 1), :128], result[64 * k : 64 * (k + 1), 128:]], axis=0)
        for k in range(4)
    ]
    sort_v[...] = dot(place, jnp.concatenate(roles, axis=1))
    for r in range(ROWS):
        send1[r] = sort_v[4 * r : 4 * r + 4, :128].astype(BF16)
        send2[r] = sort_v[4 * r : 4 * r + 4, 128:256].astype(BF16)
    recv1[pl.ds(row, 1)] = send1[pl.ds(row, 1)]
    recv2[pl.ds(row, 1)] = send2[pl.ds(row, 1)]
    end_row = lax.broadcasted_iota(jnp.int32, (16, 256), 0)
    end_col = lax.broadcasted_iota(jnp.int32, (16, 256), 1)
    ends = jnp.where(end_col == 255 * end_row, 1.0, 0.0).astype(BF16)
    edge_out[...] = dot_nt(ends, result[128:]).astype(BF16)
    loads[5].wait()
    loads[6].wait()

    def to_row(trip, r):
        source, target, sent, received = trip
        return pltpu.make_async_remote_copy(
            src_ref=source.at[r], dst_ref=target.at[row], send_sem=sent, recv_sem=received,
            device_id=(r, col), device_id_type=MESH,
        )

    def whole(trip):
        source, target, sent, received = trip
        count = pl.ds(0, source.shape[0] - 1)
        return pltpu.make_async_remote_copy(
            src_ref=source.at[count], dst_ref=target.at[count], send_sem=sent, recv_sem=received,
            device_id=(partner, col), device_id_type=MESH,
        )

    def to_relay(trip, relay, i):
        source, _, sent, _ = trip
        held, received = relay
        up = i < 4
        away = 8 - i if up else 11 - i
        sign = 1 if up else -1
        return pltpu.make_async_remote_copy(
            src_ref=source.at[pl.ds(lax.rem(z + 16 + sign * away, 16) * 2, 2)], dst_ref=held.at[pl.ds(2 * i, 2)],
            send_sem=sent, recv_sem=received, device_id=(lax.rem(z + 16 + sign * 4, 16) * 2 + core, col),
            device_id_type=MESH,
        )

    def from_relay(trip, relay, sent, i, k):
        _, target, _, received = trip
        up = i < 4
        away = 4 - i if up else 7 - i
        sign = 1 if up else -1
        origin = lax.rem(z + 16 - sign * 4, 16) * 2 + core
        return pltpu.make_async_remote_copy(
            src_ref=relay[0].at[2 * i + k], dst_ref=target.at[origin], send_sem=sent, recv_sem=received,
            device_id=(lax.rem(z + 16 + sign * away, 16) * 2 + k, col), device_id_type=MESH,
        )

    def passed(relay, sent):
        held, received = relay
        return pltpu.make_async_remote_copy(
            src_ref=held, dst_ref=held, send_sem=sent, recv_sem=received,
            device_id=(partner, col), device_id_type=MESH,
        )

    relay_order = (0, 4, 1, 5, 2, 6, 3)

    def edge(step, slot):
        return pltpu.make_async_remote_copy(
            src_ref=edge_out, dst_ref=edge_in.at[slot], send_sem=edge_send.at[slot], recv_sem=edge_recv.at[slot],
            device_id=(lax.rem(row + step, ROWS), col), device_id_type=MESH,
        )

    after_me, before_me = edge(1, 0), edge(ROWS - 1, 1)

    def block(part, step):
        if part == 0:
            return w_full.at[core, 0, y, lax.rem(x + step, 4)]
        return w_full.at[core, 1, lax.rem(y + step, 4), x]

    def group(part, step, half=None):
        some = slice(None) if half is None else pl.ds(2 * half, 2)
        if part == 0:
            return w_full.at[core, 0, lax.rem(y + step, 4), some]
        return w_full.at[core, 1, some, lax.rem(x + step, 4)]

    def along(part, step):
        return y * 4 + lax.rem(x + step, 4) if part == 0 else lax.rem(y + step, 4) * 4 + x

    def spread_block(part, step):
        here = block(part, 0)
        return pltpu.make_async_remote_copy(
            src_ref=here, dst_ref=here, send_sem=block_send.at[part, step],
            recv_sem=block_recv.at[part, step], device_id=(row, along(part, step)), device_id_type=MESH,
        )

    def hop_block(part, side, step):
        here = block(part, step)
        return pltpu.make_async_remote_copy(
            src_ref=here, dst_ref=here, send_sem=hop_send.at[part, side], recv_sem=hop_recv.at[part, side],
            device_id=(row, along(1 - part, 1 + 2 * side)), device_id_type=MESH,
        )

    def hopped(part, side):
        here = group(part, 3 - 2 * side)
        return pltpu.make_async_remote_copy(
            src_ref=here, dst_ref=here, send_sem=hop_send.at[part, side], recv_sem=hop_recv.at[part, side],
            device_id=(row, along(1 - part, 1 + 2 * side)), device_id_type=MESH,
        )

    def pass_on(part, side):
        here = group(part, 3 - 2 * side, side)
        return pltpu.make_async_remote_copy(
            src_ref=here, dst_ref=here, send_sem=pass_send.at[part, side], recv_sem=pass_recv.at[part, side],
            device_id=(row, along(1 - part, 1 + 2 * side)), device_id_type=MESH,
        )

    both = [(part, side) for part in range(2) for side in range(2)]

    def swap(part, step):
        here = group(part, step)
        return pltpu.make_async_remote_copy(
            src_ref=here, dst_ref=here, send_sem=swap_send, recv_sem=swap_recv,
            device_id=(partner, col), device_id_type=MESH,
        )

    value_trip = (send1, recv1, send_sem1, recv_sem1)
    first_trip = (send2, recv2, send_sem2, recv_sem2)
    back_trip = (send3, recv3, send_sem3, recv_sem3)
    last_trip = (send4, recv4, send_sem4, recv_sem4.at[0])
    value_relay = (relay1, relay_recv.at[0])
    first_relay = (relay2, relay_recv.at[1])

    for load in loads[7:]:
        load.wait()
    scaled = embed_v[...] * freq_v[...]
    est[...] = jnp.zeros_like(est)
    high = scaled.astype(BF16).astype(F32)
    rest = scaled - high
    mid = rest.astype(BF16).astype(F32)
    low = rest - mid
    for k, parts in enumerate(((high, high, high), (mid, mid), (low,))):
        for m, part in enumerate(parts):
            est[k, FEAT_STEP * m : FEAT_STEP * m + FEATS, :64] = part
    layer = jnp.concatenate([jnp.transpose(est[k])[:64] for k in range(3)], axis=0).astype(BF16)

    lane64 = lax.broadcasted_iota(jnp.int32, (8, 64), 1)
    sub64 = lax.broadcasted_iota(jnp.int32, (8, 64), 0)
    own_proj = jnp.zeros((8, 64), F32)
    for o in range(2):
        for d in range(2):
            pick = jnp.where((lane64 == 2 * row + (sub64 & 1)) & ((sub64 >> 1) == 2 * o + d), 1.0, 0.0)
            own_proj = own_proj + dot_nt(pick, proj_v[:, o, d, :], lax.Precision.HIGHEST)
    proj_high, proj_low = split(own_proj)
    proj_both = jnp.concatenate([own_proj, own_proj - proj_high.astype(F32)], axis=0).astype(BF16)

    def own(ref):
        lanes = lax.broadcasted_iota(jnp.int32, ref.shape, len(ref.shape) - 1)
        return [jnp.sum(jnp.where(lanes == 2 * row + c, ref[...], 0.0), axis=-1, keepdims=True) for c in range(2)]

    own_taps = own(taps_v)
    own_decay = own(decay_v)
    own_gain = own(gain_v)
    sub8 = lax.broadcasted_iota(jnp.int32, (8, 128), 0)
    decay_rows = jnp.zeros((8, 128), F32)
    start_rows = jnp.zeros((8, 128), F32)
    for o in range(2):
        for c in range(2):
            start_rows = jnp.where(sub8 == 4 * o + c, own_gain[c][o : o + 1], start_rows)
            for d in range(2):
                decay_rows = jnp.where(sub8 == 4 * o + 2 * d + c, own_decay[c][o, d : d + 1], decay_rows)
    lag8 = lax.broadcasted_iota(jnp.int32, (8, 128), 1)
    keep = ((sub8 >> 1) & 1) == 0

    def lags(step, carry):
        width = 1024
        block = table_v[:, pl.ds(pl.multiple_of(step * width, width), width)]
        parts = dot(layer, block)
        hidden = sine(parts[:64] + parts[64:128] + parts[128:])
        hid_high, hid_low = split(hidden)
        twice = dot(proj_both, hid_high)
        taps = twice[:8] + twice[8:] + dot(proj_high, hid_low)
        for i in range(width // 128):
            at = step * width + i * 128 + lag8
            piece = taps[:, 128 * i : 128 * (i + 1)] * jnp.exp(decay_rows * (at.astype(F32) * (-1.0 / (LENGTH - 1))))
            piece = jnp.where(at == 0, jnp.where(keep, piece + start_rows, 0.0), piece)
            to = ((i % 2) * 32 + i // 2 + step * 4) * 8
            lag_taps[pl.ds(pl.multiple_of(to, 8), 8), :] = piece
        return carry

    lax.fori_loop(0, LENGTH // 2048, lags, 0)

    pl.semaphore_wait(barrier, 17 + COLS - 1)
    for i in relay_order:
        to_relay(value_trip, value_relay, i).start()
    near_peers(lambda r: to_row(value_trip, r).start())
    for step in (1, 3, 2):
        for part in range(2):
            spread_block(part, step).start()
    for part, side in both:
        hop_block(part, side, 0).start()
    for i in relay_order:
        to_relay(first_trip, first_relay, i).start()
    near_peers(lambda r: to_row(first_trip, r).start())
    after_me.start()
    before_me.start()

    lax.fori_loop(LENGTH // 2048, LENGTH // 1024, lags, 0)

    for trip, relay, sent in (
        (value_trip, value_relay, relay_send.at[0]),
        (first_trip, first_relay, relay_send.at[1]),
    ):
        passed(relay, sent).wait_recv()
        for i in relay_order:
            for k in range(2):
                from_relay(trip, relay, sent, i, k).start()


    twist = (twist_v[0], twist_v[1])
    inner_in = (inner_in_v[0], inner_in_v[1])
    inner_out = (inner_out_v[0], inner_out_v[1])
    for o in range(2):
        signals = jnp.concatenate([lag_taps[pl.ds(4 * o + k, 64, stride=8), :] for k in range(4)], axis=1)
        spectra[o] = filter_spectrum(signals, outer_in_v[...], twist, inner_in)
    tables = (outer_in_v[...], outer_out_v[...], twist, inner_in, inner_out)

    for step in (1, 3, 2):
        for part in range(2):
            spread_block(part, step).wait_recv()
        for part, side in both:
            hop_block(part, side, 4 - step).start()
    for part in range(2):
        swap(part, 0).start()

    lane = lax.broadcasted_iota(jnp.int32, (32, 128), 1)
    sub = lax.broadcasted_iota(jnp.int32, (32, 128), 0)

    def arrived(buffer):
        for r in range(ROWS):
            block_v[4 * r : 4 * r + 4, :] = buffer[r].astype(F32)

    def short(role):
        sides = []
        for c in range(2):
            here = [block_v[pl.ds(2 * c + h, 32, stride=4), :] for h in range(2)]
            before, after = shifted(here, lane, sub)
            weight = [own_taps[c][j, role : role + 1] for j in range(3)]
            sides.append(
                jnp.concatenate(
                    [before[h] * weight[0] + here[h] * weight[1] + after[h] * weight[2] for h in range(2)], axis=0
                )
            )
        return jnp.concatenate(sides, axis=1)

    whole(value_trip).wait_recv()
    arrived(recv1)
    conv = convolve(short(0), spectra[0], tables)
    whole(first_trip).wait_recv()
    arrived(recv2)
    conv = convolve(short(1) * conv, spectra[1], tables)

    for c in range(2):
        for h in range(2):
            back_v[pl.ds(2 * c + h, 32, stride=4), :] = conv[32 * h : 32 * (h + 1), 128 * c : 128 * (c + 1)]
    for r in range(ROWS):
        send3[r] = back_v[4 * r : 4 * r + 4, :].astype(BF16)
    recv3[pl.ds(row, 1)] = send3[pl.ds(row, 1)]
    row_peers(lambda r: to_row(back_trip, r).start())

    lane = lax.broadcasted_iota(jnp.int32, (128, 128), 1)
    sub = lax.broadcasted_iota(jnp.int32, (128, 128), 0)
    upper = (sub & 1) == 1
    after_me.wait_recv()
    before_me.wait_recv()
    double = jnp.where(lane == (sub >> 1), 1.0, 0.0)
    edge_before = dot_nt(double.astype(BF16), edge_in[0])[:, 1:2]
    edge_after = dot_nt(double.astype(BF16), edge_in[1])[:, 0:1]
    edge_before = jnp.where(row == 0, 0.0, edge_before)
    edge_after = jnp.where(row == ROWS - 1, 0.0, edge_after)
    role_taps = jnp.concatenate([taps_v[j, 2:3] for j in range(3)] + [jnp.zeros((5, 64), F32)], axis=0)
    columns = dot_nt(double[:, :64], role_taps, lax.Precision.HIGHEST)
    here = sort_v[:, 256:384]
    right, left = pltpu.roll(here, 1, 1), pltpu.roll(here, 127, 1)
    before = jnp.where(lane == 0, jnp.where(upper, pltpu.roll(right, 1, 0), edge_before), right)
    after = jnp.where(lane == 127, jnp.where(upper, edge_after, pltpu.roll(left, 127, 0)), left)
    second = before * columns[:, 0:1] + here * columns[:, 1:2] + after * columns[:, 2:3]
    gate = sort_v[:, 384:]
    gate_v[...] = second * (gate / (1.0 + jnp.exp(-gate)))

    for part, side in both:
        hopped(part, side).wait_recv()
    for part, side in both:
        pass_on(part, side).start()
    for part in range(2):
        for step in (1, 3):
            swap(part, step).start()

    p128 = lax.broadcasted_iota(jnp.int32, (128, 256), 0)
    l256 = lax.broadcasted_iota(jnp.int32, (128, 256), 1)
    spread = jnp.where((l256 >> 7 == (p128 & 1)) & ((l256 & 63) == (p128 >> 1)), 1.0, 0.0).astype(BF16)
    whole(back_trip).wait_recv()
    arrived(recv3)
    flipped = jnp.transpose(block_v[...] * gate_v[...]).astype(BF16)
    rows = dot(flipped, spread)
    low_first = (lax.broadcasted_iota(jnp.int32, (8, 8, 128), 2) < 64) == (lax.rem(col, 2) == 0)
    for h in range(2):
        tiles = rows[:, 128 * h : 128 * (h + 1)].reshape(8, 2, 8, 128)
        send4[8 * h : 8 * (h + 1)] = jnp.where(low_first, tiles[:, 0], tiles[:, 1]).astype(BF16)
    recv4[pl.ds(col, 1)] = send4[pl.ds(col, 1)]

    def last(step_y, step_x):
        c = lax.rem(y + step_y, 4) * 4 + lax.rem(x + step_x, 4)
        return pltpu.make_async_remote_copy(
            src_ref=send4.at[c], dst_ref=recv4.at[col], send_sem=send_sem4, recv_sem=recv_sem4.at[(4 - step_y) % 4],
            device_id=(row, c), device_id_type=MESH,
        )

    def last_group(step_y):
        some = recv4.at[pl.ds(0, 4 if step_y else 3)]
        return pltpu.make_async_remote_copy(
            src_ref=some, dst_ref=some, send_sem=send_sem4, recv_sem=recv_sem4.at[step_y],
            device_id=(partner, col), device_id_type=MESH,
        )

    for step_y in (2, 1, 3, 0):
        for step_x in (2, 1, 3, 0):
            if step_y or step_x:
                last(step_y, step_x).start()

    for part, side in both:
        pass_on(part, side).wait_recv()
    for part in range(2):
        swap(part, 2).start()
    half = w_full.at[core]
    swapped = pltpu.make_async_remote_copy(
        src_ref=half, dst_ref=half, send_sem=swap_send, recv_sem=swap_recv,
        device_id=(partner, col), device_id_type=MESH,
    )
    swapped.wait_recv()
    low_lanes = lax.broadcasted_iota(jnp.int32, (8, 128), 1) < 64
    for step_y in (0, 1, 3, 2):
        last_group(step_y).wait_recv()
        yy = lax.rem(y + step_y, 4)
        lefts = []
        for m in range(2):
            even, odd = (recv4[4 * yy + 2 * m + e].astype(F32) for e in range(2))
            upper_rows = jnp.where(low_lanes, even, odd)
            lower_rows = pltpu.roll(jnp.where(low_lanes, odd, even), 64, 1)
            lefts.append(jnp.concatenate([upper_rows, lower_rows], axis=0))
        left = jnp.concatenate(lefts, axis=1).astype(BF16)
        for k in range(2):
            for part in range(2):
                at = 1024 * k + 512 * part
                term = dot(left, w_full[k, part, yy].reshape(256, 512))
                if step_y:
                    term = term + total[:, at : at + 512]
                if step_y == 2:
                    out_ref[0, :, at : at + 512] = term.astype(BF16)
                else:
                    total[:, at : at + 512] = term

    for trip in (value_trip, first_trip, back_trip, last_trip):
        whole(trip).wait_send()
    passed(value_relay, relay_send.at[0]).wait_send()
    passed(first_relay, relay_send.at[1]).wait_send()
    after_me.wait_send()
    before_me.wait_send()
    for part in range(2):
        for step in (1, 2, 3):
            spread_block(part, step).wait_send()
    for part, side in both:
        hopped(part, side).wait_send()
        pass_on(part, side).wait_send()
    swapped.wait_send()


def body(
    tokens, w_value, w_first, w_second, w_gate, conv_taps, filter_embed, filter_freq, filter_proj, filter_decay,
    skip_gain, w_out,
):
    consts = [jnp.asarray(c) for c in constants()]
    vmem = pltpu.VMEM
    sem = pltpu.SemaphoreType.DMA
    scratch = [
        vmem((256, 2048), BF16),
        vmem((256, 2048), BF16),
        vmem((3, 3, 64), F32),
        vmem((FEATS, 64), F32),
        vmem((1, 64), F32),
        vmem((64, 2, 2, 64), F32),
        vmem((2, 2, 64), F32),
        vmem((2, 64), F32),
        vmem((128, 192), BF16),
        vmem((64, 384), BF16),
        vmem((2, 64, 128), F32),
        vmem((2, 256, 256), BF16),
        vmem((2, 256, 256), BF16),
        vmem((128, LENGTH), BF16),
        vmem((2, 2, 4, 4, 64, 512), BF16),
        vmem((3, 128, 128), F32),
        vmem((512, 128), F32),
        vmem((2, 128, 256), F32),
        vmem((128, 512), F32),
        vmem((128, 128), F32),
        vmem((128, 128), F32),
        vmem((128, 128), F32),
        vmem((16, 128), BF16),
        vmem((2, 16, 128), BF16),
        vmem((ROWS, 4, 128), BF16), vmem((ROWS, 4, 128), BF16),
        vmem((ROWS, 4, 128), BF16), vmem((ROWS, 4, 128), BF16),
        vmem((ROWS, 4, 128), BF16), vmem((ROWS, 4, 128), BF16),
        vmem((COLS, 8, 128), BF16), vmem((COLS, 8, 128), BF16),
        vmem((16, 2048), F32),
        vmem((14, 4, 128), BF16), vmem((14, 4, 128), BF16),
        sem((19,)),
        sem, sem, sem, sem, sem, sem, sem, sem((4,)),
        sem((2,)), sem((2,)), sem((2, 4)), sem((2, 4)), sem((2, 2)), sem((2, 2)), sem((2, 2)), sem((2, 2)), sem, sem,
        sem((2,)), sem((2,)),
    ]
    anywhere = pl.BlockSpec(memory_space=pltpu.HBM)
    return pl.pallas_call(
        kernel,
        out_shape=jax.ShapeDtypeStruct((1, 16, 2048), BF16),
        in_specs=[anywhere] * 18,
        out_specs=pl.BlockSpec(memory_space=pltpu.VMEM),
        scratch_shapes=scratch,
        compiler_params=pltpu.CompilerParams(
            collective_id=0, has_side_effects=True, vmem_limit_bytes=48 * 1024 * 1024
        ),
    )(*[
        pltpu.with_memory_space_constraint(operand, pltpu.HBM)
        for operand in (
            tokens, w_value.T, w_first.T, w_second.T, w_gate.T, conv_taps, filter_embed, filter_freq.reshape(1, -1),
            filter_proj, filter_decay, skip_gain, w_out, *consts,
        )
    ])


def solution(mesh):
    placed = (
        P(None, "row", None),
        P(None, "col"),
        P(None, "col"),
        P(None, "col"),
        P(None, "col"),
        P(None, None, "col"),
        P(),
        P(),
        P(None, None, None, "col"),
        P(None, None, "col"),
        P(None, "col"),
        P("col", None),
    )
    return jax.shard_map(
        body, mesh=mesh, in_specs=placed, out_specs=P(None, ("row", "col"), None), check_vma=False
    )
```

```python
import functools
import math

import jax
import jax.numpy as jnp
import ml_dtypes
import numpy as np
from jax import lax
from jax.experimental import pallas as pl
from jax.experimental.pallas import tpu as pltpu
from jax.sharding import PartitionSpec as P

MESH = pl.DeviceIdType.MESH
F32 = jnp.float32
BF16 = jnp.bfloat16

LENGTH = 8192
ROWS = 32
COLS = 16
FEATS = 33
FEAT_STEP = 40


def halves(x):
    x = np.asarray(x, np.float64)
    high = x.astype(ml_dtypes.bfloat16)
    low = (x - high.astype(np.float64)).astype(ml_dtypes.bfloat16)
    return high, low


@functools.lru_cache(None)
def constants():
    two_pi = 2.0 * math.pi
    j = np.arange(64)
    q = 2 * (j % 32) + j // 32
    k1 = np.arange(64) + 0.5
    p = np.arange(128)
    first = np.concatenate([np.cos(two_pi * np.outer(k1, q) / 128), -np.sin(two_pi * np.outer(k1, q) / 128)], axis=0)
    f_high, f_low = halves(first)
    outer_in = np.concatenate([f_high, f_high, f_low], axis=1)
    outer_out = np.concatenate([f_high.T, f_high.T, f_low.T], axis=1)
    twist = np.stack(
        [np.cos(two_pi * np.outer(k1, p) / 16384), -np.sin(two_pi * np.outer(k1, p) / 16384)]
    ).astype(np.float32)
    g_real = np.cos(two_pi * (np.outer(p, p) % 128) / 128)
    g_imag = -np.sin(two_pi * (np.outer(p, p) % 128) / 128)
    inner_in = np.stack(halves(np.block([[g_real, g_imag], [-g_imag, g_real]])))
    inner_out = np.stack(halves(np.block([[g_real, -g_imag], [g_imag, g_real]])))
    n = np.arange(LENGTH)
    b = np.arange(1, 17)
    phase = two_pi * (np.outer(b, n) % LENGTH) / LENGTH
    features = np.concatenate([(n / (LENGTH - 1))[None], np.cos(phase), np.sin(phase)], axis=0)
    table = np.zeros((128, LENGTH), ml_dtypes.bfloat16)
    rest = features
    for part in range(3):
        piece = rest.astype(ml_dtypes.bfloat16)
        table[part * FEAT_STEP : part * FEAT_STEP + FEATS] = piece
        rest = rest - piece.astype(np.float64)
    return outer_in, outer_out, twist, inner_in, inner_out, table


def split(x):
    high = x.astype(BF16)
    return high, (x - high.astype(F32)).astype(BF16)


def dot(a, b):
    return jnp.dot(a, b, preferred_element_type=F32)


def dot_nt(a, b, precision=None):
    return lax.dot_general(a, b, (((1,), (1,)), ((), ())), precision=precision, preferred_element_type=F32)


def times(x, matrix):
    high, low = split(x)
    return dot(high, matrix[0]) + dot(low, matrix[0]) + dot(high, matrix[1])


def forward(signal, outer_in, twist, inner_in):
    high, low = split(signal)
    stage = dot(outer_in, jnp.concatenate([high, low, high], axis=0))
    turned = []
    for m in range(signal.shape[1] // 128):
        real = stage[:64, 128 * m : 128 * (m + 1)]
        imag = stage[64:, 128 * m : 128 * (m + 1)]
        turned.append(
            jnp.concatenate([real * twist[0] - imag * twist[1], real * twist[1] + imag * twist[0]], axis=1)
        )
    return times(jnp.concatenate(turned, axis=0), inner_in)


def inverse(spectrum, outer_out, twist, inner_out):
    stage = times(spectrum, inner_out)
    reals, imags = [], []
    for m in range(spectrum.shape[0] // 64):
        real = stage[64 * m : 64 * (m + 1), :128]
        imag = stage[64 * m : 64 * (m + 1), 128:]
        reals.append(real * twist[0] + imag * twist[1])
        imags.append(imag * twist[0] - real * twist[1])
    both = jnp.concatenate([jnp.concatenate(reals, axis=1), jnp.concatenate(imags, axis=1)], axis=0)
    high, low = split(both)
    return dot(outer_out, jnp.concatenate([high, low, high], axis=0))


def convolve(signal, filt, tables):
    outer_in, outer_out, twist, inner_in, inner_out = tables
    spectrum = forward(signal, outer_in, twist, inner_in)
    real, imag = spectrum[:, :128], spectrum[:, 128:]
    f_real, f_imag = filt[:, :128], filt[:, 128:]
    product = jnp.concatenate([real * f_real - imag * f_imag, real * f_imag + imag * f_real], axis=1)
    return inverse(product, outer_out, twist, inner_out)


def filter_spectrum(signals, outer_in, twist, inner_in):
    spectra = forward(signals, outer_in, twist, inner_in)
    ahead, behind = spectra[:128], spectra[128:]
    scale = 2.0 / (2 * LENGTH)
    return jnp.concatenate(
        [(ahead[:, :128] + behind[:, :128]) * scale, (ahead[:, 128:] - behind[:, 128:]) * scale], axis=1
    )


def sine(x):
    k = jnp.floor(x * (1.0 / math.pi) + 0.5)
    r = x - k * 3.140625
    r = r - k * 9.67502593994140625e-4
    r = r - k * 1.509957990978376432e-7
    half = k * 0.5
    sign = 1.0 - 4.0 * (half - jnp.floor(half))
    s = r * r
    poly = -1.0 / 39916800.0
    for c in (1.0 / 362880.0, -1.0 / 5040.0, 1.0 / 120.0, -1.0 / 6.0):
        poly = poly * s + c
    return sign * (r + r * (s * poly))


def shifted(parts, lane, sub):
    right = [pltpu.roll(x, 1, 1) for x in parts]
    left = [pltpu.roll(x, 127, 1) for x in parts]
    carry = jnp.where(sub == 0, 0.0, pltpu.roll(right[1], 1, 0))
    back = jnp.where(sub == 31, 0.0, pltpu.roll(left[0], 31, 0))
    before = [jnp.where(lane == 0, carry, right[0]), jnp.where(lane == 0, right[0], right[1])]
    after = [jnp.where(lane == 127, left[1], left[0]), jnp.where(lane == 127, back, left[1])]
    return before, after


def kernel(
    tokens, w_value, w_first, w_second, w_gate, conv_taps, embed, freq, proj, decay, gain, w_out,
    outer_in_h, outer_out_h, twist_h, inner_in_h, inner_out_h, table_h,
    out_ref,
    tok_v, w_v, taps_v, embed_v, freq_v, proj_v, decay_v, gain_v,
    outer_in_v, outer_out_v, twist_v, inner_in_v, inner_out_v, table_v,
    w_full, est, lag_taps, spectra, sort_v, gate_v, block_v, back_v, edge_out, edge_in,
    send1, recv1, send2, recv2, send3, recv3, send4, recv4, total, relay1, relay2,
    load_sem, send_sem1, recv_sem1, send_sem2, recv_sem2, send_sem3, recv_sem3, send_sem4, recv_sem4,
    edge_send, edge_recv, block_send, block_recv, hop_send, hop_recv, pass_send, pass_recv, swap_send, swap_recv,
    relay_send, relay_recv,
):
    row = lax.axis_index("row")
    col = lax.axis_index("col")
    z = lax.div(row, 2)
    core = lax.rem(row, 2)
    partner = z * 2 + 1 - core
    y = lax.div(col, 4)
    x = lax.rem(col, 4)

    def row_peers(visit):
        def step(i, carry):
            away = 8 + lax.div(i + 1, 2) * (1 - 2 * lax.rem(i, 2))
            there = lax.rem(z + away, 16) * 2
            visit(there)
            visit(there + 1)
            return carry

        lax.fori_loop(0, 15, step, 0)
        visit(partner)

    def near_peers(visit):
        def step(i, carry):
            away = 4 - lax.div(i, 2)
            there = lax.rem(z + 16 + away * (1 - 2 * lax.rem(i, 2)), 16) * 2
            visit(there)
            visit(there + 1)
            return carry

        lax.fori_loop(0, 8, step, 0)
        visit(partner)

    def col_peers(visit):
        def step(i, carry):
            visit(lax.rem(col + i, COLS))
            return carry

        lax.fori_loop(1, COLS, step, 0)

    barrier = pltpu.get_barrier_semaphore()
    near_peers(lambda r: pl.semaphore_signal(barrier, inc=1, device_id=(r, col), device_id_type=MESH))
    col_peers(lambda c: pl.semaphore_signal(barrier, inc=1, device_id=(row, c), device_id_type=MESH))

    loads = []
    for source, target in (
        (tokens.at[0], tok_v),
        (w_value, w_v.at[pl.ds(0, 64)]),
        (w_first, w_v.at[pl.ds(64, 64)]),
        (w_second, w_v.at[pl.ds(128, 64)]),
        (w_gate, w_v.at[pl.ds(192, 64)]),
        (w_out.at[:, pl.ds(pl.multiple_of(core * 1024, 512), 512)], w_full.at[core, 0, y, x]),
        (w_out.at[:, pl.ds(pl.multiple_of(core * 1024 + 512, 512), 512)], w_full.at[core, 1, y, x]),
        (conv_taps, taps_v),
        (embed, embed_v),
        (freq, freq_v),
        (proj, proj_v),
        (decay, decay_v),
        (gain, gain_v),
        (table_h, table_v),
        (outer_in_h, outer_in_v),
        (outer_out_h, outer_out_v),
        (twist_h, twist_v),
        (inner_in_h, inner_in_v),
        (inner_out_h, inner_out_v),
    ):
        load = pltpu.make_async_copy(source, target, load_sem.at[len(loads)])
        load.start()
        loads.append(load)

    for load in loads[:5]:
        load.wait()
    result = dot_nt(w_v[...], tok_v[...]).astype(BF16)
    order = lax.broadcasted_iota(jnp.int32, (128, 128), 0)
    source = lax.broadcasted_iota(jnp.int32, (128, 128), 1)
    place = jnp.where(source == (order & 1) * 64 + (order >> 1), 1.0, 0.0).astype(BF16)
    roles = [
        jnp.concatenate([result[64 * k : 64 * (k + 1), :128], result[64 * k : 64 * (k + 1), 128:]], axis=0)
        for k in range(4)
    ]
    sort_v[...] = dot(place, jnp.concatenate(roles, axis=1))
    for r in range(ROWS):
        send1[r] = sort_v[4 * r : 4 * r + 4, :128].astype(BF16)
        send2[r] = sort_v[4 * r : 4 * r + 4, 128:256].astype(BF16)
    recv1[pl.ds(row, 1)] = send1[pl.ds(row, 1)]
    recv2[pl.ds(row, 1)] = send2[pl.ds(row, 1)]
    end_row = lax.broadcasted_iota(jnp.int32, (16, 256), 0)
    end_col = lax.broadcasted_iota(jnp.int32, (16, 256), 1)
    ends = jnp.where(end_col == 255 * end_row, 1.0, 0.0).astype(BF16)
    edge_out[...] = dot_nt(ends, result[128:]).astype(BF16)
    loads[5].wait()
    loads[6].wait()

    def to_row(trip, r):
        source, target, sent, received = trip
        return pltpu.make_async_remote_copy(
            src_ref=source.at[r], dst_ref=target.at[row], send_sem=sent, recv_sem=received,
            device_id=(r, col), device_id_type=MESH,
        )

    def whole(trip):
        source, target, sent, received = trip
        count = pl.ds(0, source.shape[0] - 1)
        return pltpu.make_async_remote_copy(
            src_ref=source.at[count], dst_ref=target.at[count], send_sem=sent, recv_sem=received,
            device_id=(partner, col), device_id_type=MESH,
        )

    def to_relay(trip, relay, i):
        source, _, sent, _ = trip
        held, received = relay
        up = i < 4
        away = 8 - i if up else 11 - i
        sign = 1 if up else -1
        return pltpu.make_async_remote_copy(
            src_ref=source.at[pl.ds(lax.rem(z + 16 + sign * away, 16) * 2, 2)], dst_ref=held.at[pl.ds(2 * i, 2)],
            send_sem=sent, recv_sem=received, device_id=(lax.rem(z + 16 + sign * 4, 16) * 2 + core, col),
            device_id_type=MESH,
        )

    def from_relay(trip, relay, sent, i, k):
        _, target, _, received = trip
        up = i < 4
        away = 4 - i if up else 7 - i
        sign = 1 if up else -1
        origin = lax.rem(z + 16 - sign * 4, 16) * 2 + core
        return pltpu.make_async_remote_copy(
            src_ref=relay[0].at[2 * i + k], dst_ref=target.at[origin], send_sem=sent, recv_sem=received,
            device_id=(lax.rem(z + 16 + sign * away, 16) * 2 + k, col), device_id_type=MESH,
        )

    def passed(relay, sent):
        held, received = relay
        return pltpu.make_async_remote_copy(
            src_ref=held, dst_ref=held, send_sem=sent, recv_sem=received,
            device_id=(partner, col), device_id_type=MESH,
        )

    relay_order = (0, 4, 1, 5, 2, 6, 3)

    def edge(step, slot):
        return pltpu.make_async_remote_copy(
            src_ref=edge_out, dst_ref=edge_in.at[slot], send_sem=edge_send.at[slot], recv_sem=edge_recv.at[slot],
            device_id=(lax.rem(row + step, ROWS), col), device_id_type=MESH,
        )

    after_me, before_me = edge(1, 0), edge(ROWS - 1, 1)

    def block(part, step):
        if part == 0:
            return w_full.at[core, 0, y, lax.rem(x + step, 4)]
        return w_full.at[core, 1, lax.rem(y + step, 4), x]

    def group(part, step, half=None):
        some = slice(None) if half is None else pl.ds(2 * half, 2)
        if part == 0:
            return w_full.at[core, 0, lax.rem(y + step, 4), some]
        return w_full.at[core, 1, some, lax.rem(x + step, 4)]

    def along(part, step):
        return y * 4 + lax.rem(x + step, 4) if part == 0 else lax.rem(y + step, 4) * 4 + x

    def spread_block(part, step):
        here = block(part, 0)
        return pltpu.make_async_remote_copy(
            src_ref=here, dst_ref=here, send_sem=block_send.at[part, step],
            recv_sem=block_recv.at[part, step], device_id=(row, along(part, step)), device_id_type=MESH,
        )

    def hop_block(part, side, step):
        here = block(part, step)
        return pltpu.make_async_remote_copy(
            src_ref=here, dst_ref=here, send_sem=hop_send.at[part, side], recv_sem=hop_recv.at[part, side],
            device_id=(row, along(1 - part, 1 + 2 * side)), device_id_type=MESH,
        )

    def hopped(part, side):
        here = group(part, 3 - 2 * side)
        return pltpu.make_async_remote_copy(
            src_ref=here, dst_ref=here, send_sem=hop_send.at[part, side], recv_sem=hop_recv.at[part, side],
            device_id=(row, along(1 - part, 1 + 2 * side)), device_id_type=MESH,
        )

    def pass_on(part, side):
        here = group(part, 3 - 2 * side, side)
        return pltpu.make_async_remote_copy(
            src_ref=here, dst_ref=here, send_sem=pass_send.at[part, side], recv_sem=pass_recv.at[part, side],
            device_id=(row, along(1 - part, 1 + 2 * side)), device_id_type=MESH,
        )

    both = [(part, side) for part in range(2) for side in range(2)]

    def swap(part, step):
        here = group(part, step)
        return pltpu.make_async_remote_copy(
            src_ref=here, dst_ref=here, send_sem=swap_send, recv_sem=swap_recv,
            device_id=(partner, col), device_id_type=MESH,
        )

    value_trip = (send1, recv1, send_sem1, recv_sem1)
    first_trip = (send2, recv2, send_sem2, recv_sem2)
    back_trip = (send3, recv3, send_sem3, recv_sem3)
    last_trip = (send4, recv4, send_sem4, recv_sem4.at[0])
    value_relay = (relay1, relay_recv.at[0])
    first_relay = (relay2, relay_recv.at[1])

    pl.semaphore_wait(barrier, 17 + COLS - 1)
    for i in relay_order:
        to_relay(value_trip, value_relay, i).start()
    near_peers(lambda r: to_row(value_trip, r).start())
    for step in (1, 3, 2):
        for part in range(2):
            spread_block(part, step).start()
    for part, side in both:
        hop_block(part, side, 0).start()
    for i in relay_order:
        to_relay(first_trip, first_relay, i).start()
    near_peers(lambda r: to_row(first_trip, r).start())
    after_me.start()
    before_me.start()

    for load in loads[7:]:
        load.wait()
    scaled = embed_v[...] * freq_v[...]
    est[...] = jnp.zeros_like(est)
    high = scaled.astype(BF16).astype(F32)
    rest = scaled - high
    mid = rest.astype(BF16).astype(F32)
    low = rest - mid
    for k, parts in enumerate(((high, high, high), (mid, mid), (low,))):
        for m, part in enumerate(parts):
            est[k, FEAT_STEP * m : FEAT_STEP * m + FEATS, :64] = part
    layer = jnp.concatenate([jnp.transpose(est[k])[:64] for k in range(3)], axis=0).astype(BF16)

    lane64 = lax.broadcasted_iota(jnp.int32, (8, 64), 1)
    sub64 = lax.broadcasted_iota(jnp.int32, (8, 64), 0)
    own_proj = jnp.zeros((8, 64), F32)
    for o in range(2):
        for d in range(2):
            pick = jnp.where((lane64 == 2 * row + (sub64 & 1)) & ((sub64 >> 1) == 2 * o + d), 1.0, 0.0)
            own_proj = own_proj + dot_nt(pick, proj_v[:, o, d, :], lax.Precision.HIGHEST)
    proj_high, proj_low = split(own_proj)
    proj_both = jnp.concatenate([own_proj, own_proj - proj_high.astype(F32)], axis=0).astype(BF16)

    def own(ref):
        lanes = lax.broadcasted_iota(jnp.int32, ref.shape, len(ref.shape) - 1)
        return [jnp.sum(jnp.where(lanes == 2 * row + c, ref[...], 0.0), axis=-1, keepdims=True) for c in range(2)]

    own_taps = own(taps_v)
    own_decay = own(decay_v)
    own_gain = own(gain_v)
    sub8 = lax.broadcasted_iota(jnp.int32, (8, 128), 0)
    decay_rows = jnp.zeros((8, 128), F32)
    start_rows = jnp.zeros((8, 128), F32)
    for o in range(2):
        for c in range(2):
            start_rows = jnp.where(sub8 == 4 * o + c, own_gain[c][o : o + 1], start_rows)
            for d in range(2):
                decay_rows = jnp.where(sub8 == 4 * o + 2 * d + c, own_decay[c][o, d : d + 1], decay_rows)
    lag8 = lax.broadcasted_iota(jnp.int32, (8, 128), 1)
    keep = ((sub8 >> 1) & 1) == 0

    def lags(step, carry):
        width = 1024
        block = table_v[:, pl.ds(pl.multiple_of(step * width, width), width)]
        parts = dot(layer, block)
        hidden = sine(parts[:64] + parts[64:128] + parts[128:])
        hid_high, hid_low = split(hidden)
        twice = dot(proj_both, hid_high)
        taps = twice[:8] + twice[8:] + dot(proj_high, hid_low)
        for i in range(width // 128):
            at = step * width + i * 128 + lag8
            piece = taps[:, 128 * i : 128 * (i + 1)] * jnp.exp(decay_rows * (at.astype(F32) * (-1.0 / (LENGTH - 1))))
            piece = jnp.where(at == 0, jnp.where(keep, piece + start_rows, 0.0), piece)
            to = ((i % 2) * 32 + i // 2 + step * 4) * 8
            lag_taps[pl.ds(pl.multiple_of(to, 8), 8), :] = piece
        return carry

    lax.fori_loop(0, 6, lags, 0)

    for trip, relay, sent in (
        (value_trip, value_relay, relay_send.at[0]),
        (first_trip, first_relay, relay_send.at[1]),
    ):
        passed(relay, sent).wait_recv()
        for i in relay_order:
            for k in range(2):
                from_relay(trip, relay, sent, i, k).start()


    lax.fori_loop(6, 8, lags, 0)

    twist = (twist_v[0], twist_v[1])
    inner_in = (inner_in_v[0], inner_in_v[1])
    inner_out = (inner_out_v[0], inner_out_v[1])
    for o in range(2):
        signals = jnp.concatenate([lag_taps[pl.ds(4 * o + k, 64, stride=8), :] for k in range(4)], axis=1)
        spectra[o] = filter_spectrum(signals, outer_in_v[...], twist, inner_in)
    tables = (outer_in_v[...], outer_out_v[...], twist, inner_in, inner_out)

    for step in (1, 3, 2):
        for part in range(2):
            spread_block(part, step).wait_recv()
        for part, side in both:
            hop_block(part, side, 4 - step).start()
    for part in range(2):
        swap(part, 0).start()

    lane = lax.broadcasted_iota(jnp.int32, (32, 128), 1)
    sub = lax.broadcasted_iota(jnp.int32, (32, 128), 0)

    def arrived(buffer):
        for r in range(ROWS):
            block_v[4 * r : 4 * r + 4, :] = buffer[r].astype(F32)

    def short(role):
        sides = []
        for c in range(2):
            here = [block_v[pl.ds(2 * c + h, 32, stride=4), :] for h in range(2)]
            before, after = shifted(here, lane, sub)
            weight = [own_taps[c][j, role : role + 1] for j in range(3)]
            sides.append(
                jnp.concatenate(
                    [before[h] * weight[0] + here[h] * weight[1] + after[h] * weight[2] for h in range(2)], axis=0
                )
            )
        return jnp.concatenate(sides, axis=1)

    whole(value_trip).wait_recv()
    arrived(recv1)
    conv = convolve(short(0), spectra[0], tables)
    whole(first_trip).wait_recv()
    arrived(recv2)
    conv = convolve(short(1) * conv, spectra[1], tables)

    for c in range(2):
        for h in range(2):
            back_v[pl.ds(2 * c + h, 32, stride=4), :] = conv[32 * h : 32 * (h + 1), 128 * c : 128 * (c + 1)]
    for r in range(ROWS):
        send3[r] = back_v[4 * r : 4 * r + 4, :].astype(BF16)
    recv3[pl.ds(row, 1)] = send3[pl.ds(row, 1)]
    row_peers(lambda r: to_row(back_trip, r).start())

    lane = lax.broadcasted_iota(jnp.int32, (128, 128), 1)
    sub = lax.broadcasted_iota(jnp.int32, (128, 128), 0)
    upper = (sub & 1) == 1
    after_me.wait_recv()
    before_me.wait_recv()
    double = jnp.where(lane == (sub >> 1), 1.0, 0.0)
    edge_before = dot_nt(double.astype(BF16), edge_in[0])[:, 1:2]
    edge_after = dot_nt(double.astype(BF16), edge_in[1])[:, 0:1]
    edge_before = jnp.where(row == 0, 0.0, edge_before)
    edge_after = jnp.where(row == ROWS - 1, 0.0, edge_after)
    role_taps = jnp.concatenate([taps_v[j, 2:3] for j in range(3)] + [jnp.zeros((5, 64), F32)], axis=0)
    columns = dot_nt(double[:, :64], role_taps, lax.Precision.HIGHEST)
    here = sort_v[:, 256:384]
    right, left = pltpu.roll(here, 1, 1), pltpu.roll(here, 127, 1)
    before = jnp.where(lane == 0, jnp.where(upper, pltpu.roll(right, 1, 0), edge_before), right)
    after = jnp.where(lane == 127, jnp.where(upper, edge_after, pltpu.roll(left, 127, 0)), left)
    second = before * columns[:, 0:1] + here * columns[:, 1:2] + after * columns[:, 2:3]
    gate = sort_v[:, 384:]
    gate_v[...] = second * (gate / (1.0 + jnp.exp(-gate)))

    for part, side in both:
        hopped(part, side).wait_recv()
    for part, side in both:
        pass_on(part, side).start()
    for part in range(2):
        for step in (1, 3):
            swap(part, step).start()

    p128 = lax.broadcasted_iota(jnp.int32, (128, 256), 0)
    l256 = lax.broadcasted_iota(jnp.int32, (128, 256), 1)
    spread = jnp.where((l256 >> 7 == (p128 & 1)) & ((l256 & 63) == (p128 >> 1)), 1.0, 0.0).astype(BF16)
    whole(back_trip).wait_recv()
    arrived(recv3)
    flipped = jnp.transpose(block_v[...] * gate_v[...]).astype(BF16)
    rows = dot(flipped, spread)
    low_first = (lax.broadcasted_iota(jnp.int32, (8, 8, 128), 2) < 64) == (lax.rem(col, 2) == 0)
    for h in range(2):
        tiles = rows[:, 128 * h : 128 * (h + 1)].reshape(8, 2, 8, 128)
        send4[8 * h : 8 * (h + 1)] = jnp.where(low_first, tiles[:, 0], tiles[:, 1]).astype(BF16)
    recv4[pl.ds(col, 1)] = send4[pl.ds(col, 1)]

    def last(step_y, step_x):
        c = lax.rem(y + step_y, 4) * 4 + lax.rem(x + step_x, 4)
        return pltpu.make_async_remote_copy(
            src_ref=send4.at[c], dst_ref=recv4.at[col], send_sem=send_sem4, recv_sem=recv_sem4.at[(4 - step_y) % 4],
            device_id=(row, c), device_id_type=MESH,
        )

    def last_group(step_y):
        some = recv4.at[pl.ds(0, 4 if step_y else 3)]
        return pltpu.make_async_remote_copy(
            src_ref=some, dst_ref=some, send_sem=send_sem4, recv_sem=recv_sem4.at[step_y],
            device_id=(partner, col), device_id_type=MESH,
        )

    for step_y in (2, 1, 3, 0):
        for step_x in (2, 1, 3, 0):
            if step_y or step_x:
                last(step_y, step_x).start()

    for part, side in both:
        pass_on(part, side).wait_recv()
    for part in range(2):
        swap(part, 2).start()
    half = w_full.at[core]
    swapped = pltpu.make_async_remote_copy(
        src_ref=half, dst_ref=half, send_sem=swap_send, recv_sem=swap_recv,
        device_id=(partner, col), device_id_type=MESH,
    )
    swapped.wait_recv()
    low_lanes = lax.broadcasted_iota(jnp.int32, (8, 128), 1) < 64
    for step_y in (0, 1, 3, 2):
        last_group(step_y).wait_recv()
        yy = lax.rem(y + step_y, 4)
        lefts = []
        for m in range(2):
            even, odd = (recv4[4 * yy + 2 * m + e].astype(F32) for e in range(2))
            upper_rows = jnp.where(low_lanes, even, odd)
            lower_rows = pltpu.roll(jnp.where(low_lanes, odd, even), 64, 1)
            lefts.append(jnp.concatenate([upper_rows, lower_rows], axis=0))
        left = jnp.concatenate(lefts, axis=1).astype(BF16)
        for k in range(2):
            for part in range(2):
                at = 1024 * k + 512 * part
                term = dot(left, w_full[k, part, yy].reshape(256, 512))
                if step_y:
                    term = term + total[:, at : at + 512]
                if step_y == 2:
                    out_ref[0, :, at : at + 512] = term.astype(BF16)
                else:
                    total[:, at : at + 512] = term

    for trip in (value_trip, first_trip, back_trip, last_trip):
        whole(trip).wait_send()
    passed(value_relay, relay_send.at[0]).wait_send()
    passed(first_relay, relay_send.at[1]).wait_send()
    after_me.wait_send()
    before_me.wait_send()
    for part in range(2):
        for step in (1, 2, 3):
            spread_block(part, step).wait_send()
    for part, side in both:
        hopped(part, side).wait_send()
        pass_on(part, side).wait_send()
    swapped.wait_send()


def body(
    tokens, w_value, w_first, w_second, w_gate, conv_taps, filter_embed, filter_freq, filter_proj, filter_decay,
    skip_gain, w_out,
):
    consts = [jnp.asarray(c) for c in constants()]
    vmem = pltpu.VMEM
    sem = pltpu.SemaphoreType.DMA
    scratch = [
        vmem((256, 2048), BF16),
        vmem((256, 2048), BF16),
        vmem((3, 3, 64), F32),
        vmem((FEATS, 64), F32),
        vmem((1, 64), F32),
        vmem((64, 2, 2, 64), F32),
        vmem((2, 2, 64), F32),
        vmem((2, 64), F32),
        vmem((128, 192), BF16),
        vmem((64, 384), BF16),
        vmem((2, 64, 128), F32),
        vmem((2, 256, 256), BF16),
        vmem((2, 256, 256), BF16),
        vmem((128, LENGTH), BF16),
        vmem((2, 2, 4, 4, 64, 512), BF16),
        vmem((3, 128, 128), F32),
        vmem((512, 128), F32),
        vmem((2, 128, 256), F32),
        vmem((128, 512), F32),
        vmem((128, 128), F32),
        vmem((128, 128), F32),
        vmem((128, 128), F32),
        vmem((16, 128), BF16),
        vmem((2, 16, 128), BF16),
        vmem((ROWS, 4, 128), BF16), vmem((ROWS, 4, 128), BF16),
        vmem((ROWS, 4, 128), BF16), vmem((ROWS, 4, 128), BF16),
        vmem((ROWS, 4, 128), BF16), vmem((ROWS, 4, 128), BF16),
        vmem((COLS, 8, 128), BF16), vmem((COLS, 8, 128), BF16),
        vmem((16, 2048), F32),
        vmem((14, 4, 128), BF16), vmem((14, 4, 128), BF16),
        sem((19,)),
        sem, sem, sem, sem, sem, sem, sem, sem((4,)),
        sem((2,)), sem((2,)), sem((2, 4)), sem((2, 4)), sem((2, 2)), sem((2, 2)), sem((2, 2)), sem((2, 2)), sem, sem,
        sem((2,)), sem((2,)),
    ]
    anywhere = pl.BlockSpec(memory_space=pltpu.HBM)
    return pl.pallas_call(
        kernel,
        out_shape=jax.ShapeDtypeStruct((1, 16, 2048), BF16),
        in_specs=[anywhere] * 18,
        out_specs=pl.BlockSpec(memory_space=pltpu.VMEM),
        scratch_shapes=scratch,
        compiler_params=pltpu.CompilerParams(
            collective_id=0, has_side_effects=True, vmem_limit_bytes=48 * 1024 * 1024
        ),
    )(*[
        pltpu.with_memory_space_constraint(operand, pltpu.HBM)
        for operand in (
            tokens, w_value.T, w_first.T, w_second.T, w_gate.T, conv_taps, filter_embed, filter_freq.reshape(1, -1),
            filter_proj, filter_decay, skip_gain, w_out, *consts,
        )
    ])


def solution(mesh):
    placed = (
        P(None, "row", None),
        P(None, "col"),
        P(None, "col"),
        P(None, "col"),
        P(None, "col"),
        P(None, None, "col"),
        P(),
        P(),
        P(None, None, None, "col"),
        P(None, None, "col"),
        P(None, "col"),
        P("col", None),
    )
    return jax.shard_map(
        body, mesh=mesh, in_specs=placed, out_specs=P(None, ("row", "col"), None), check_vma=False
    )
```

```python
import functools
import math

import jax
import jax.numpy as jnp
import ml_dtypes
import numpy as np
from jax import lax
from jax.experimental import pallas as pl
from jax.experimental.pallas import tpu as pltpu
from jax.sharding import PartitionSpec as P

MESH = pl.DeviceIdType.MESH
F32 = jnp.float32
BF16 = jnp.bfloat16

LENGTH = 8192
ROWS = 32
COLS = 16
FEATS = 33
FEAT_STEP = 40


def halves(x):
    x = np.asarray(x, np.float64)
    high = x.astype(ml_dtypes.bfloat16)
    low = (x - high.astype(np.float64)).astype(ml_dtypes.bfloat16)
    return high, low


@functools.lru_cache(None)
def constants():
    two_pi = 2.0 * math.pi
    j = np.arange(64)
    q = 2 * (j % 32) + j // 32
    k1 = np.arange(64) + 0.5
    p = np.arange(128)
    first = np.concatenate([np.cos(two_pi * np.outer(k1, q) / 128), -np.sin(two_pi * np.outer(k1, q) / 128)], axis=0)
    f_high, f_low = halves(first)
    outer_in = np.concatenate([f_high, f_high, f_low], axis=1)
    outer_out = np.concatenate([f_high.T, f_high.T, f_low.T], axis=1)
    twist = np.stack(
        [np.cos(two_pi * np.outer(k1, p) / 16384), -np.sin(two_pi * np.outer(k1, p) / 16384)]
    ).astype(np.float32)
    g_real = np.cos(two_pi * (np.outer(p, p) % 128) / 128)
    g_imag = -np.sin(two_pi * (np.outer(p, p) % 128) / 128)
    inner_in = np.stack(halves(np.block([[g_real, g_imag], [-g_imag, g_real]])))
    inner_out = np.stack(halves(np.block([[g_real, -g_imag], [g_imag, g_real]])))
    n = np.arange(LENGTH)
    b = np.arange(1, 17)
    phase = two_pi * (np.outer(b, n) % LENGTH) / LENGTH
    features = np.concatenate([(n / (LENGTH - 1))[None], np.cos(phase), np.sin(phase)], axis=0)
    table = np.zeros((128, LENGTH), ml_dtypes.bfloat16)
    rest = features
    for part in range(3):
        piece = rest.astype(ml_dtypes.bfloat16)
        table[part * FEAT_STEP : part * FEAT_STEP + FEATS] = piece
        rest = rest - piece.astype(np.float64)
    return outer_in, outer_out, twist, inner_in, inner_out, table


def split(x):
    high = x.astype(BF16)
    return high, (x - high.astype(F32)).astype(BF16)


def dot(a, b):
    return jnp.dot(a, b, preferred_element_type=F32)


def dot_nt(a, b, precision=None):
    return lax.dot_general(a, b, (((1,), (1,)), ((), ())), precision=precision, preferred_element_type=F32)


def times(x, matrix):
    high, low = split(x)
    return dot(high, matrix[0]) + dot(low, matrix[0]) + dot(high, matrix[1])


def forward(signal, outer_in, twist, inner_in):
    high, low = split(signal)
    stage = dot(outer_in, jnp.concatenate([high, low, high], axis=0))
    turned = []
    for m in range(signal.shape[1] // 128):
        real = stage[:64, 128 * m : 128 * (m + 1)]
        imag = stage[64:, 128 * m : 128 * (m + 1)]
        turned.append(
            jnp.concatenate([real * twist[0] - imag * twist[1], real * twist[1] + imag * twist[0]], axis=1)
        )
    return times(jnp.concatenate(turned, axis=0), inner_in)


def inverse(spectrum, outer_out, twist, inner_out):
    stage = times(spectrum, inner_out)
    reals, imags = [], []
    for m in range(spectrum.shape[0] // 64):
        real = stage[64 * m : 64 * (m + 1), :128]
        imag = stage[64 * m : 64 * (m + 1), 128:]
        reals.append(real * twist[0] + imag * twist[1])
        imags.append(imag * twist[0] - real * twist[1])
    both = jnp.concatenate([jnp.concatenate(reals, axis=1), jnp.concatenate(imags, axis=1)], axis=0)
    high, low = split(both)
    return dot(outer_out, jnp.concatenate([high, low, high], axis=0))


def convolve(signal, filt, tables):
    outer_in, outer_out, twist, inner_in, inner_out = tables
    spectrum = forward(signal, outer_in, twist, inner_in)
    real, imag = spectrum[:, :128], spectrum[:, 128:]
    f_real, f_imag = filt[:, :128], filt[:, 128:]
    product = jnp.concatenate([real * f_real - imag * f_imag, real * f_imag + imag * f_real], axis=1)
    return inverse(product, outer_out, twist, inner_out)


def filter_spectrum(signals, outer_in, twist, inner_in):
    spectra = forward(signals, outer_in, twist, inner_in)
    ahead, behind = spectra[:128], spectra[128:]
    scale = 2.0 / (2 * LENGTH)
    return jnp.concatenate(
        [(ahead[:, :128] + behind[:, :128]) * scale, (ahead[:, 128:] - behind[:, 128:]) * scale], axis=1
    )


def sine(x):
    k = jnp.floor(x * (1.0 / math.pi) + 0.5)
    r = x - k * 3.140625
    r = r - k * 9.67502593994140625e-4
    r = r - k * 1.509957990978376432e-7
    half = k * 0.5
    sign = 1.0 - 4.0 * (half - jnp.floor(half))
    s = r * r
    poly = -1.0 / 39916800.0
    for c in (1.0 / 362880.0, -1.0 / 5040.0, 1.0 / 120.0, -1.0 / 6.0):
        poly = poly * s + c
    return sign * (r + r * (s * poly))


def shifted(parts, lane, sub):
    right = [pltpu.roll(x, 1, 1) for x in parts]
    left = [pltpu.roll(x, 127, 1) for x in parts]
    carry = jnp.where(sub == 0, 0.0, pltpu.roll(right[1], 1, 0))
    back = jnp.where(sub == 31, 0.0, pltpu.roll(left[0], 31, 0))
    before = [jnp.where(lane == 0, carry, right[0]), jnp.where(lane == 0, right[0], right[1])]
    after = [jnp.where(lane == 127, left[1], left[0]), jnp.where(lane == 127, back, left[1])]
    return before, after


def kernel(
    tokens, w_value, w_first, w_second, w_gate, conv_taps, embed, freq, proj, decay, gain, w_out,
    outer_in_h, outer_out_h, twist_h, inner_in_h, inner_out_h, table_h,
    out_ref,
    tok_v, w_v, taps_v, embed_v, freq_v, proj_v, decay_v, gain_v,
    outer_in_v, outer_out_v, twist_v, inner_in_v, inner_out_v, table_v,
    w_full, est, lag_taps, spectra, sort_v, gate_v, block_v, back_v, edge_out, edge_in,
    send1, recv1, send2, recv2, send3, recv3, send4, recv4, total, relay1, relay2,
    load_sem, send_sem1, recv_sem1, send_sem2, recv_sem2, send_sem3, recv_sem3, send_sem4, recv_sem4,
    edge_send, edge_recv, block_send, block_recv, hop_send, hop_recv, pass_send, pass_recv, swap_send, swap_recv,
    relay_send, relay_recv,
):
    row = lax.axis_index("row")
    col = lax.axis_index("col")
    z = lax.div(row, 2)
    core = lax.rem(row, 2)
    partner = z * 2 + 1 - core
    y = lax.div(col, 4)
    x = lax.rem(col, 4)

    def row_peers(visit):
        def step(i, carry):
            away = 8 + lax.div(i + 1, 2) * (1 - 2 * lax.rem(i, 2))
            there = lax.rem(z + away, 16) * 2
            visit(there)
            visit(there + 1)
            return carry

        lax.fori_loop(0, 15, step, 0)
        visit(partner)

    def near_peers(visit):
        def step(i, carry):
            away = 4 - lax.div(i, 2)
            there = lax.rem(z + 16 + away * (1 - 2 * lax.rem(i, 2)), 16) * 2
            visit(there)
            visit(there + 1)
            return carry

        lax.fori_loop(0, 8, step, 0)
        visit(partner)

    def col_peers(visit):
        def step(i, carry):
            visit(lax.rem(col + i, COLS))
            return carry

        lax.fori_loop(1, COLS, step, 0)

    barrier = pltpu.get_barrier_semaphore()
    near_peers(lambda r: pl.semaphore_signal(barrier, inc=1, device_id=(r, col), device_id_type=MESH))
    col_peers(lambda c: pl.semaphore_signal(barrier, inc=1, device_id=(row, c), device_id_type=MESH))

    loads = []
    for source, target in (
        (tokens.at[0], tok_v),
        (w_value, w_v.at[pl.ds(0, 64)]),
        (w_first, w_v.at[pl.ds(64, 64)]),
        (w_second, w_v.at[pl.ds(128, 64)]),
        (w_gate, w_v.at[pl.ds(192, 64)]),
        (w_out.at[:, pl.ds(pl.multiple_of(core * 1024, 512), 512)], w_full.at[core, 0, y, x]),
        (w_out.at[:, pl.ds(pl.multiple_of(core * 1024 + 512, 512), 512)], w_full.at[core, 1, y, x]),
        (conv_taps, taps_v),
        (embed, embed_v),
        (freq, freq_v),
        (proj, proj_v),
        (decay, decay_v),
        (gain, gain_v),
        (table_h, table_v),
        (outer_in_h, outer_in_v),
        (outer_out_h, outer_out_v),
        (twist_h, twist_v),
        (inner_in_h, inner_in_v),
        (inner_out_h, inner_out_v),
    ):
        load = pltpu.make_async_copy(source, target, load_sem.at[len(loads)])
        load.start()
        loads.append(load)

    for load in loads[:5]:
        load.wait()
    result = dot_nt(w_v[...], tok_v[...]).astype(BF16)
    order = lax.broadcasted_iota(jnp.int32, (128, 128), 0)
    source = lax.broadcasted_iota(jnp.int32, (128, 128), 1)
    place = jnp.where(source == (order & 1) * 64 + (order >> 1), 1.0, 0.0).astype(BF16)
    roles = [
        jnp.concatenate([result[64 * k : 64 * (k + 1), :128], result[64 * k : 64 * (k + 1), 128:]], axis=0)
        for k in range(4)
    ]
    sort_v[...] = dot(place, jnp.concatenate(roles, axis=1))
    for r in range(ROWS):
        send1[r] = sort_v[4 * r : 4 * r + 4, :128].astype(BF16)
        send2[r] = sort_v[4 * r : 4 * r + 4, 128:256].astype(BF16)
    recv1[pl.ds(row, 1)] = send1[pl.ds(row, 1)]
    recv2[pl.ds(row, 1)] = send2[pl.ds(row, 1)]
    end_row = lax.broadcasted_iota(jnp.int32, (16, 256), 0)
    end_col = lax.broadcasted_iota(jnp.int32, (16, 256), 1)
    ends = jnp.where(end_col == 255 * end_row, 1.0, 0.0).astype(BF16)
    edge_out[...] = dot_nt(ends, result[128:]).astype(BF16)
    loads[5].wait()
    loads[6].wait()

    def to_row(trip, r):
        source, target, sent, received = trip
        return pltpu.make_async_remote_copy(
            src_ref=source.at[r], dst_ref=target.at[row], send_sem=sent, recv_sem=received,
            device_id=(r, col), device_id_type=MESH,
        )

    def whole(trip):
        source, target, sent, received = trip
        count = pl.ds(0, source.shape[0] - 1)
        return pltpu.make_async_remote_copy(
            src_ref=source.at[count], dst_ref=target.at[count], send_sem=sent, recv_sem=received,
            device_id=(partner, col), device_id_type=MESH,
        )

    def to_relay(trip, relay, i):
        source, _, sent, _ = trip
        held, received = relay
        up = i < 4
        away = 8 - i if up else 11 - i
        sign = 1 if up else -1
        return pltpu.make_async_remote_copy(
            src_ref=source.at[pl.ds(lax.rem(z + 16 + sign * away, 16) * 2, 2)], dst_ref=held.at[pl.ds(2 * i, 2)],
            send_sem=sent, recv_sem=received, device_id=(lax.rem(z + 16 + sign * 4, 16) * 2 + core, col),
            device_id_type=MESH,
        )

    def from_relay(trip, relay, sent, i, k):
        _, target, _, received = trip
        up = i < 4
        away = 4 - i if up else 7 - i
        sign = 1 if up else -1
        origin = lax.rem(z + 16 - sign * 4, 16) * 2 + core
        return pltpu.make_async_remote_copy(
            src_ref=relay[0].at[2 * i + k], dst_ref=target.at[origin], send_sem=sent, recv_sem=received,
            device_id=(lax.rem(z + 16 + sign * away, 16) * 2 + k, col), device_id_type=MESH,
        )

    def passed(relay, sent):
        held, received = relay
        return pltpu.make_async_remote_copy(
            src_ref=held, dst_ref=held, send_sem=sent, recv_sem=received,
            device_id=(partner, col), device_id_type=MESH,
        )

    relay_order = (0, 4, 1, 5, 2, 6, 3)

    def edge(step, slot):
        return pltpu.make_async_remote_copy(
            src_ref=edge_out, dst_ref=edge_in.at[slot], send_sem=edge_send.at[slot], recv_sem=edge_recv.at[slot],
            device_id=(lax.rem(row + step, ROWS), col), device_id_type=MESH,
        )

    after_me, before_me = edge(1, 0), edge(ROWS - 1, 1)

    def block(part, step):
        if part == 0:
            return w_full.at[core, 0, y, lax.rem(x + step, 4)]
        return w_full.at[core, 1, lax.rem(y + step, 4), x]

    def group(part, step, half=None):
        some = slice(None) if half is None else pl.ds(2 * half, 2)
        if part == 0:
            return w_full.at[core, 0, lax.rem(y + step, 4), some]
        return w_full.at[core, 1, some, lax.rem(x + step, 4)]

    def along(part, step):
        return y * 4 + lax.rem(x + step, 4) if part == 0 else lax.rem(y + step, 4) * 4 + x

    def spread_block(part, step):
        here = block(part, 0)
        return pltpu.make_async_remote_copy(
            src_ref=here, dst_ref=here, send_sem=block_send.at[part, step],
            recv_sem=block_recv.at[part, step], device_id=(row, along(part, step)), device_id_type=MESH,
        )

    def hop_block(part, side, step):
        here = block(part, step)
        return pltpu.make_async_remote_copy(
            src_ref=here, dst_ref=here, send_sem=hop_send.at[part, side], recv_sem=hop_recv.at[part, side],
            device_id=(row, along(1 - part, 1 + 2 * side)), device_id_type=MESH,
        )

    def hopped(part, side):
        here = group(part, 3 - 2 * side)
        return pltpu.make_async_remote_copy(
            src_ref=here, dst_ref=here, send_sem=hop_send.at[part, side], recv_sem=hop_recv.at[part, side],
            device_id=(row, along(1 - part, 1 + 2 * side)), device_id_type=MESH,
        )

    def pass_on(part, side):
        here = group(part, 3 - 2 * side, side)
        return pltpu.make_async_remote_copy(
            src_ref=here, dst_ref=here, send_sem=pass_send.at[part, side], recv_sem=pass_recv.at[part, side],
            device_id=(row, along(1 - part, 1 + 2 * side)), device_id_type=MESH,
        )

    both = [(part, side) for part in range(2) for side in range(2)]

    def swap(part, step):
        here = group(part, step)
        return pltpu.make_async_remote_copy(
            src_ref=here, dst_ref=here, send_sem=swap_send, recv_sem=swap_recv,
            device_id=(partner, col), device_id_type=MESH,
        )

    value_trip = (send1, recv1, send_sem1, recv_sem1)
    first_trip = (send2, recv2, send_sem2, recv_sem2)
    back_trip = (send3, recv3, send_sem3, recv_sem3)
    last_trip = (send4, recv4, send_sem4, recv_sem4.at[0])
    value_relay = (relay1, relay_recv.at[0])
    first_relay = (relay2, relay_recv.at[1])

    pl.semaphore_wait(barrier, 17 + COLS - 1)
    for i in relay_order:
        to_relay(value_trip, value_relay, i).start()
    near_peers(lambda r: to_row(value_trip, r).start())
    for i in relay_order:
        to_relay(first_trip, first_relay, i).start()
    for step in (1, 3, 2):
        for part in range(2):
            spread_block(part, step).start()
    for part, side in both:
        hop_block(part, side, 0).start()
    near_peers(lambda r: to_row(first_trip, r).start())
    after_me.start()
    before_me.start()

    for load in loads[7:]:
        load.wait()
    scaled = embed_v[...] * freq_v[...]
    est[...] = jnp.zeros_like(est)
    high = scaled.astype(BF16).astype(F32)
    rest = scaled - high
    mid = rest.astype(BF16).astype(F32)
    low = rest - mid
    for k, parts in enumerate(((high, high, high), (mid, mid), (low,))):
        for m, part in enumerate(parts):
            est[k, FEAT_STEP * m : FEAT_STEP * m + FEATS, :64] = part
    layer = jnp.concatenate([jnp.transpose(est[k])[:64] for k in range(3)], axis=0).astype(BF16)

    lane64 = lax.broadcasted_iota(jnp.int32, (8, 64), 1)
    sub64 = lax.broadcasted_iota(jnp.int32, (8, 64), 0)
    own_proj = jnp.zeros((8, 64), F32)
    for o in range(2):
        for d in range(2):
            pick = jnp.where((lane64 == 2 * row + (sub64 & 1)) & ((sub64 >> 1) == 2 * o + d), 1.0, 0.0)
            own_proj = own_proj + dot_nt(pick, proj_v[:, o, d, :], lax.Precision.HIGHEST)
    proj_high, proj_low = split(own_proj)
    proj_both = jnp.concatenate([own_proj, own_proj - proj_high.astype(F32)], axis=0).astype(BF16)

    def own(ref):
        lanes = lax.broadcasted_iota(jnp.int32, ref.shape, len(ref.shape) - 1)
        return [jnp.sum(jnp.where(lanes == 2 * row + c, ref[...], 0.0), axis=-1, keepdims=True) for c in range(2)]

    own_taps = own(taps_v)
    own_decay = own(decay_v)
    own_gain = own(gain_v)
    sub8 = lax.broadcasted_iota(jnp.int32, (8, 128), 0)
    decay_rows = jnp.zeros((8, 128), F32)
    start_rows = jnp.zeros((8, 128), F32)
    for o in range(2):
        for c in range(2):
            start_rows = jnp.where(sub8 == 4 * o + c, own_gain[c][o : o + 1], start_rows)
            for d in range(2):
                decay_rows = jnp.where(sub8 == 4 * o + 2 * d + c, own_decay[c][o, d : d + 1], decay_rows)
    lag8 = lax.broadcasted_iota(jnp.int32, (8, 128), 1)
    keep = ((sub8 >> 1) & 1) == 0

    def lags(step, carry):
        width = 1024
        block = table_v[:, pl.ds(pl.multiple_of(step * width, width), width)]
        parts = dot(layer, block)
        hidden = sine(parts[:64] + parts[64:128] + parts[128:])
        hid_high, hid_low = split(hidden)
        twice = dot(proj_both, hid_high)
        taps = twice[:8] + twice[8:] + dot(proj_high, hid_low)
        for i in range(width // 128):
            at = step * width + i * 128 + lag8
            piece = taps[:, 128 * i : 128 * (i + 1)] * jnp.exp(decay_rows * (at.astype(F32) * (-1.0 / (LENGTH - 1))))
            piece = jnp.where(at == 0, jnp.where(keep, piece + start_rows, 0.0), piece)
            to = ((i % 2) * 32 + i // 2 + step * 4) * 8
            lag_taps[pl.ds(pl.multiple_of(to, 8), 8), :] = piece
        return carry

    lax.fori_loop(0, 6, lags, 0)

    for trip, relay, sent in (
        (value_trip, value_relay, relay_send.at[0]),
        (first_trip, first_relay, relay_send.at[1]),
    ):
        passed(relay, sent).wait_recv()
        for i in relay_order:
            for k in range(2):
                from_relay(trip, relay, sent, i, k).start()


    lax.fori_loop(6, 8, lags, 0)

    twist = (twist_v[0], twist_v[1])
    inner_in = (inner_in_v[0], inner_in_v[1])
    inner_out = (inner_out_v[0], inner_out_v[1])
    for o in range(2):
        signals = jnp.concatenate([lag_taps[pl.ds(4 * o + k, 64, stride=8), :] for k in range(4)], axis=1)
        spectra[o] = filter_spectrum(signals, outer_in_v[...], twist, inner_in)
    tables = (outer_in_v[...], outer_out_v[...], twist, inner_in, inner_out)

    for step in (1, 3, 2):
        for part in range(2):
            spread_block(part, step).wait_recv()
        for part, side in both:
            hop_block(part, side, 4 - step).start()
    for part in range(2):
        swap(part, 0).start()

    lane = lax.broadcasted_iota(jnp.int32, (32, 128), 1)
    sub = lax.broadcasted_iota(jnp.int32, (32, 128), 0)

    def arrived(buffer):
        for r in range(ROWS):
            block_v[4 * r : 4 * r + 4, :] = buffer[r].astype(F32)

    def short(role):
        sides = []
        for c in range(2):
            here = [block_v[pl.ds(2 * c + h, 32, stride=4), :] for h in range(2)]
            before, after = shifted(here, lane, sub)
            weight = [own_taps[c][j, role : role + 1] for j in range(3)]
            sides.append(
                jnp.concatenate(
                    [before[h] * weight[0] + here[h] * weight[1] + after[h] * weight[2] for h in range(2)], axis=0
                )
            )
        return jnp.concatenate(sides, axis=1)

    whole(value_trip).wait_recv()
    arrived(recv1)
    conv = convolve(short(0), spectra[0], tables)
    whole(first_trip).wait_recv()
    arrived(recv2)
    conv = convolve(short(1) * conv, spectra[1], tables)

    for c in range(2):
        for h in range(2):
            back_v[pl.ds(2 * c + h, 32, stride=4), :] = conv[32 * h : 32 * (h + 1), 128 * c : 128 * (c + 1)]
    for r in range(ROWS):
        send3[r] = back_v[4 * r : 4 * r + 4, :].astype(BF16)
    recv3[pl.ds(row, 1)] = send3[pl.ds(row, 1)]
    row_peers(lambda r: to_row(back_trip, r).start())

    lane = lax.broadcasted_iota(jnp.int32, (128, 128), 1)
    sub = lax.broadcasted_iota(jnp.int32, (128, 128), 0)
    upper = (sub & 1) == 1
    after_me.wait_recv()
    before_me.wait_recv()
    double = jnp.where(lane == (sub >> 1), 1.0, 0.0)
    edge_before = dot_nt(double.astype(BF16), edge_in[0])[:, 1:2]
    edge_after = dot_nt(double.astype(BF16), edge_in[1])[:, 0:1]
    edge_before = jnp.where(row == 0, 0.0, edge_before)
    edge_after = jnp.where(row == ROWS - 1, 0.0, edge_after)
    role_taps = jnp.concatenate([taps_v[j, 2:3] for j in range(3)] + [jnp.zeros((5, 64), F32)], axis=0)
    columns = dot_nt(double[:, :64], role_taps, lax.Precision.HIGHEST)
    here = sort_v[:, 256:384]
    right, left = pltpu.roll(here, 1, 1), pltpu.roll(here, 127, 1)
    before = jnp.where(lane == 0, jnp.where(upper, pltpu.roll(right, 1, 0), edge_before), right)
    after = jnp.where(lane == 127, jnp.where(upper, edge_after, pltpu.roll(left, 127, 0)), left)
    second = before * columns[:, 0:1] + here * columns[:, 1:2] + after * columns[:, 2:3]
    gate = sort_v[:, 384:]
    gate_v[...] = second * (gate / (1.0 + jnp.exp(-gate)))

    for part, side in both:
        hopped(part, side).wait_recv()
    for part, side in both:
        pass_on(part, side).start()
    for part in range(2):
        for step in (1, 3):
            swap(part, step).start()

    p128 = lax.broadcasted_iota(jnp.int32, (128, 256), 0)
    l256 = lax.broadcasted_iota(jnp.int32, (128, 256), 1)
    spread = jnp.where((l256 >> 7 == (p128 & 1)) & ((l256 & 63) == (p128 >> 1)), 1.0, 0.0).astype(BF16)
    whole(back_trip).wait_recv()
    arrived(recv3)
    flipped = jnp.transpose(block_v[...] * gate_v[...]).astype(BF16)
    rows = dot(flipped, spread)
    low_first = (lax.broadcasted_iota(jnp.int32, (8, 8, 128), 2) < 64) == (lax.rem(col, 2) == 0)
    for h in range(2):
        tiles = rows[:, 128 * h : 128 * (h + 1)].reshape(8, 2, 8, 128)
        send4[8 * h : 8 * (h + 1)] = jnp.where(low_first, tiles[:, 0], tiles[:, 1]).astype(BF16)
    recv4[pl.ds(col, 1)] = send4[pl.ds(col, 1)]

    def last(step_y, step_x):
        c = lax.rem(y + step_y, 4) * 4 + lax.rem(x + step_x, 4)
        return pltpu.make_async_remote_copy(
            src_ref=send4.at[c], dst_ref=recv4.at[col], send_sem=send_sem4, recv_sem=recv_sem4.at[(4 - step_y) % 4],
            device_id=(row, c), device_id_type=MESH,
        )

    def last_group(step_y):
        some = recv4.at[pl.ds(0, 4 if step_y else 3)]
        return pltpu.make_async_remote_copy(
            src_ref=some, dst_ref=some, send_sem=send_sem4, recv_sem=recv_sem4.at[step_y],
            device_id=(partner, col), device_id_type=MESH,
        )

    for step_y in (2, 1, 3, 0):
        for step_x in (2, 1, 3, 0):
            if step_y or step_x:
                last(step_y, step_x).start()

    for part, side in both:
        pass_on(part, side).wait_recv()
    for part in range(2):
        swap(part, 2).start()
    half = w_full.at[core]
    swapped = pltpu.make_async_remote_copy(
        src_ref=half, dst_ref=half, send_sem=swap_send, recv_sem=swap_recv,
        device_id=(partner, col), device_id_type=MESH,
    )
    swapped.wait_recv()
    low_lanes = lax.broadcasted_iota(jnp.int32, (8, 128), 1) < 64
    for step_y in (0, 1, 3, 2):
        last_group(step_y).wait_recv()
        yy = lax.rem(y + step_y, 4)
        lefts = []
        for m in range(2):
            even, odd = (recv4[4 * yy + 2 * m + e].astype(F32) for e in range(2))
            upper_rows = jnp.where(low_lanes, even, odd)
            lower_rows = pltpu.roll(jnp.where(low_lanes, odd, even), 64, 1)
            lefts.append(jnp.concatenate([upper_rows, lower_rows], axis=0))
        left = jnp.concatenate(lefts, axis=1).astype(BF16)
        for k in range(2):
            for part in range(2):
                at = 1024 * k + 512 * part
                term = dot(left, w_full[k, part, yy].reshape(256, 512))
                if step_y:
                    term = term + total[:, at : at + 512]
                if step_y == 2:
                    out_ref[0, :, at : at + 512] = term.astype(BF16)
                else:
                    total[:, at : at + 512] = term

    for trip in (value_trip, first_trip, back_trip, last_trip):
        whole(trip).wait_send()
    passed(value_relay, relay_send.at[0]).wait_send()
    passed(first_relay, relay_send.at[1]).wait_send()
    after_me.wait_send()
    before_me.wait_send()
    for part in range(2):
        for step in (1, 2, 3):
            spread_block(part, step).wait_send()
    for part, side in both:
        hopped(part, side).wait_send()
        pass_on(part, side).wait_send()
    swapped.wait_send()


def body(
    tokens, w_value, w_first, w_second, w_gate, conv_taps, filter_embed, filter_freq, filter_proj, filter_decay,
    skip_gain, w_out,
):
    consts = [jnp.asarray(c) for c in constants()]
    vmem = pltpu.VMEM
    sem = pltpu.SemaphoreType.DMA
    scratch = [
        vmem((256, 2048), BF16),
        vmem((256, 2048), BF16),
        vmem((3, 3, 64), F32),
        vmem((FEATS, 64), F32),
        vmem((1, 64), F32),
        vmem((64, 2, 2, 64), F32),
        vmem((2, 2, 64), F32),
        vmem((2, 64), F32),
        vmem((128, 192), BF16),
        vmem((64, 384), BF16),
        vmem((2, 64, 128), F32),
        vmem((2, 256, 256), BF16),
        vmem((2, 256, 256), BF16),
        vmem((128, LENGTH), BF16),
        vmem((2, 2, 4, 4, 64, 512), BF16),
        vmem((3, 128, 128), F32),
        vmem((512, 128), F32),
        vmem((2, 128, 256), F32),
        vmem((128, 512), F32),
        vmem((128, 128), F32),
        vmem((128, 128), F32),
        vmem((128, 128), F32),
        vmem((16, 128), BF16),
        vmem((2, 16, 128), BF16),
        vmem((ROWS, 4, 128), BF16), vmem((ROWS, 4, 128), BF16),
        vmem((ROWS, 4, 128), BF16), vmem((ROWS, 4, 128), BF16),
        vmem((ROWS, 4, 128), BF16), vmem((ROWS, 4, 128), BF16),
        vmem((COLS, 8, 128), BF16), vmem((COLS, 8, 128), BF16),
        vmem((16, 2048), F32),
        vmem((14, 4, 128), BF16), vmem((14, 4, 128), BF16),
        sem((19,)),
        sem, sem, sem, sem, sem, sem, sem, sem((4,)),
        sem((2,)), sem((2,)), sem((2, 4)), sem((2, 4)), sem((2, 2)), sem((2, 2)), sem((2, 2)), sem((2, 2)), sem, sem,
        sem((2,)), sem((2,)),
    ]
    anywhere = pl.BlockSpec(memory_space=pltpu.HBM)
    return pl.pallas_call(
        kernel,
        out_shape=jax.ShapeDtypeStruct((1, 16, 2048), BF16),
        in_specs=[anywhere] * 18,
        out_specs=pl.BlockSpec(memory_space=pltpu.VMEM),
        scratch_shapes=scratch,
        compiler_params=pltpu.CompilerParams(
            collective_id=0, has_side_effects=True, vmem_limit_bytes=48 * 1024 * 1024
        ),
    )(*[
        pltpu.with_memory_space_constraint(operand, pltpu.HBM)
        for operand in (
            tokens, w_value.T, w_first.T, w_second.T, w_gate.T, conv_taps, filter_embed, filter_freq.reshape(1, -1),
            filter_proj, filter_decay, skip_gain, w_out, *consts,
        )
    ])


def solution(mesh):
    placed = (
        P(None, "row", None),
        P(None, "col"),
        P(None, "col"),
        P(None, "col"),
        P(None, "col"),
        P(None, None, "col"),
        P(),
        P(),
        P(None, None, None, "col"),
        P(None, None, "col"),
        P(None, "col"),
        P("col", None),
    )
    return jax.shard_map(
        body, mesh=mesh, in_specs=placed, out_specs=P(None, ("row", "col"), None), check_vma=False
    )
```
